32 devices in a mesh: sp: 8 (over z, x), tp: 4 (over y, core).
Axes of the slice: x: 2, y: 2, z: 4, core: 2. Of those that a mesh axis runs over, the one named last changes fastest.
Arguments:
- tokens: bfloat16 [6144, 2048], P(('sp', 'tp')), may hold values from -6 to 6
- in_gain: float32 [2048], replicated, may hold values from 0.1 to 1.9
- w_query: bfloat16 [2048, 1024], P(None, 'tp'), may hold values from -0.125 to 0.125
- w_key: bfloat16 [2048, 1024], P(None, 'tp'), may hold values from -0.125 to 0.125
- w_value: bfloat16 [2048, 2048], P(None, 'tp'), may hold values from -0.125 to 0.125
- w_input_gate: bfloat16 [2048, 8], replicated, may hold values from -8 to 8
- w_forget_gate: bfloat16 [2048, 8], replicated, may hold values from -0.125 to 0.125
- forget_bias: float32 [8], replicated
- forget_extra: float32 [6144, 8], P('sp', 'tp'), may hold values from -2 to 0
- w_conv_gate: bfloat16 [2048, 2048], P(None, 'tp'), may hold values from -0.125 to 0.125
- w_conv_left: bfloat16 [2048, 2048], P(None, 'tp'), may hold values from -0.125 to 0.125
- w_conv_right: bfloat16 [2048, 2048], P(None, 'tp'), may hold values from -0.125 to 0.125
- conv_taps: float32 [3, 2048], replicated, may hold values from -3.5 to 3.5
- first_memory: float32 [8, 128, 256], P('tp'), may hold values from -2560 to 2560
- first_norm: float32 [8, 128], P('tp'), may hold values from -2560 to 2560
- w_out_memory: bfloat16 [2048, 2048], P('tp'), may hold values from -0.09375 to 0.09375
- w_out_conv: bfloat16 [2048, 2048], P('tp'), may hold values from -0.09375 to 0.09375
Outputs:
- mixed: bfloat16 [6144, 2048], P(('sp', 'tp'))
The draws below stay inside these ranges and needn't reach their ends.
All inputs are finite; a program needn't handle non-finite values.
Results may differ from the reference program's by a relative error of at most 0.015.
The reference program's roundings to bfloat16 on the way count: a program that leaves them out, or rounds other values in their place, can miss the bound.
Values may be sent and summed in bfloat16 or wider, within the bound.
A program may use at most 64 MiB of HBM per device.

```python
import math
import jax
import jax.numpy as jnp
from jax import lax

D = 2048
MEMORY_HEADS = 8
KEY_DIM = 128
VALUE_DIM = 256
CONV_CH = 2048
TAPS = 3
TOK_DEV = 768
SEQUENCE_TOKENS = 6144
QK_WIDTH = 1024
V_WIDTH = 2048
N_TP = 4


def decay_plan(key):
    base_key = jax.random.fold_in(key, 7)
    order_key, spread_key, block_key, place_key, loss_key = jax.random.split(base_key, 5)
    fast_heads = jax.random.permutation(order_key, MEMORY_HEADS) < MEMORY_HEADS // 2
    spread = jax.random.uniform(spread_key, (MEMORY_HEADS,), jnp.float32)
    head_bias = jnp.where(fast_heads, 4.0 + 1.5 * spread, math.log(SEQUENCE_TOKENS) + 1.5 + spread)
    return (head_bias, block_key, place_key, loss_key)


def draw_forget_bias(key, part):
    head_bias, block_key, place_key, loss_key = decay_plan(key)
    return head_bias.astype(jnp.float32)


def draw_forget_extra(key, part):
    head_bias, block_key, place_key, loss_key = decay_plan(key)
    head_rate = jnp.exp(-head_bias)
    factor = jax.random.uniform(block_key, (SEQUENCE_TOKENS // TOK_DEV, MEMORY_HEADS), jnp.float32, 0.0, 2.0)
    block_portion = -jnp.repeat(factor, TOK_DEV, axis=0) * head_rate[None, :]
    place_slots = jax.random.randint(place_key, (3, MEMORY_HEADS), 0, SEQUENCE_TOKENS)
    loss_values = jnp.log(jax.random.uniform(loss_key, (3, MEMORY_HEADS), jnp.float32, 0.6, 0.8))
    token_positions = jnp.arange(SEQUENCE_TOKENS, dtype=jnp.int32)
    span_total_sum = jnp.zeros((SEQUENCE_TOKENS, MEMORY_HEADS), jnp.float32)
    for token_span in range(3):
        span_total_sum = span_total_sum + jnp.where(token_positions[:, None] == place_slots[token_span][None, :], loss_values[token_span][None, :], 0.0)
    return (block_portion + span_total_sum).astype(jnp.float32)


def draw_w_input_gate(key, part):
    weights = jax.random.normal(jax.random.fold_in(key, 11), (D, MEMORY_HEADS), jnp.float32) / math.sqrt(D)
    return jnp.clip(weights, -8.0, 8.0).astype(jnp.bfloat16)


def steps_of(key, extent, cuts, least, top_value):
    loudness, own = 1.0, jax.random.fold_in(key, 6)
    for position, blocks in cuts:
        heights = jnp.exp(jax.random.uniform(jax.random.fold_in(own, position), (blocks,), jnp.float32, least / len(cuts), top_value / len(cuts)))
        loudness = loudness * jnp.repeat(heights, extent[position] // blocks).reshape([-1 if axis == position else 1 for axis in range(len(extent))])
    return loudness


def noise(own_key, shape, scale, bound, pieces=(), held_as=jnp.bfloat16):
    drawn = jax.random.normal(own_key, shape, jnp.float32) * scale
    if len(pieces) > 0:
        drawn = steps_of(own_key, shape, pieces, -0.22, 0.18) * drawn
    return jnp.clip(drawn, min=-bound, max=bound).astype(held_as)


def setup_inputs(seed: int = 0) -> dict:
    splits = jax.random.split(jax.random.key(seed), 18)
    return {
        "tokens": noise(splits[0], (SEQUENCE_TOKENS, D), 1.0, 6.0, ((0, 32),)),
        "in_gain": jnp.clip(1.0 + 0.18 * jax.random.normal(splits[1], (D,), jnp.float32), 0.1, 1.9),
        "w_query": noise(splits[2], (D, QK_WIDTH), D ** -0.5, 0.125, ((1, 4),)),
        "w_key": noise(splits[3], (D, QK_WIDTH), D ** -0.5, 0.125, ((1, 4),)),
        "w_value": noise(splits[4], (D, V_WIDTH), D ** -0.5, 0.125, ((1, 4),)),
        "w_input_gate": draw_w_input_gate(jax.random.fold_in(splits[17], 71), 0),
        "w_forget_gate": noise(splits[6], (D, MEMORY_HEADS), D ** -0.5, 0.125),
        "forget_bias": draw_forget_bias(jax.random.fold_in(splits[17], 71), 0),
        "forget_extra": draw_forget_extra(jax.random.fold_in(splits[17], 71), 0),
        "w_conv_gate": noise(splits[9], (D, CONV_CH), D ** -0.5, 0.125, ((1, 4),)),
        "w_conv_left": noise(splits[10], (D, CONV_CH), D ** -0.5, 0.125, ((1, 4),)),
        "w_conv_right": noise(splits[11], (D, CONV_CH), D ** -0.5, 0.125, ((1, 4),)),
        "conv_taps": noise(splits[12], (TAPS, CONV_CH), TAPS ** -0.5, 3.5, (), jnp.float32),
        "first_memory": noise(splits[13], (MEMORY_HEADS, KEY_DIM, VALUE_DIM), (6 * SEQUENCE_TOKENS ** 0.5), 2560.0, ((0, 4),), jnp.float32),
        "first_norm": noise(splits[14], (MEMORY_HEADS, KEY_DIM), (6 * SEQUENCE_TOKENS ** 0.5), 2560.0, ((0, 4),), jnp.float32),
        "w_out_memory": noise(splits[15], (V_WIDTH, D), (V_WIDTH + CONV_CH) ** -0.5, 0.09375, ((0, 4),)),
        "w_out_conv": noise(splits[16], (CONV_CH, D), (V_WIDTH + CONV_CH) ** -0.5, 0.09375, ((0, 4),)),
    }


epsilon = 1e-06

def rounded(values):
    return lax.optimization_barrier(values.astype(jnp.bfloat16)).astype(jnp.float32)

def mixer_block(carried_state, inputs):
    carry_max, carry_memory, carry_norm = carried_state
    query_rows, key_rows, value_rows, in_pre, log_forget = inputs
    length = query_rows.shape[0]
    query_scale = KEY_DIM ** (-0.5)
    cumulative = jnp.cumsum(log_forget, axis=0)
    decay_total = cumulative[length - 1]
    weight_log = decay_total[None, :] - cumulative + in_pre
    block_max = lax.optimization_barrier(jnp.max(weight_log, axis=0))
    keyed = key_rows.astype(jnp.float32) * jnp.exp(weight_log - block_max[None, :])[:, :, None]
    block_norm = lax.optimization_barrier(jnp.sum(keyed, axis=0))
    block_memory = jnp.einsum('shd,shv->hdv', rounded(keyed), value_rows.astype(jnp.float32))
    token_positions = jnp.arange(length, dtype=jnp.int32)
    causal = token_positions[:, None] >= token_positions[None, :]
    cum_heads = cumulative.T
    log_gap = cum_heads[:, :, None] - cum_heads[:, None, :] + in_pre.T[:, None, :]
    log_gap = jnp.where(causal[None], log_gap, -jnp.inf)
    inter_log = cum_heads + carry_max[:, None]
    row_max = jnp.maximum(inter_log, lax.optimization_barrier(jnp.max(log_gap, axis=2)))
    raw_scores = jnp.einsum('thd,shd->hts', query_rows.astype(jnp.float32), key_rows.astype(jnp.float32)) * query_scale
    mixing = raw_scores * jnp.exp(log_gap - row_max[:, :, None])
    carried = jnp.exp(inter_log - row_max).T
    scaled_query = query_rows.astype(jnp.float32) * query_scale
    from_values = jnp.einsum('hts,shv->thv', rounded(mixing), value_rows.astype(jnp.float32))
    from_memory = jnp.einsum('thd,hdv->thv', scaled_query, carry_memory, precision=lax.Precision.HIGHEST)
    from_norm = jnp.einsum('thd,hd->th', scaled_query, carry_norm, precision=lax.Precision.HIGHEST)
    numerator = from_values + carried[:, :, None] * from_memory
    denominator = lax.optimization_barrier(jnp.sum(mixing, axis=2)).T + carried * from_norm
    memory_out = numerator / jnp.maximum(jnp.abs(denominator), 1.0)[:, :, None]
    row_mean = lax.optimization_barrier(jnp.mean(memory_out * memory_out, axis=(1, 2), keepdims=True))
    heads_out = (memory_out * lax.rsqrt(row_mean + epsilon)).astype(jnp.bfloat16)
    new_max = jnp.maximum(carry_max + decay_total, block_max)
    old_scale = jnp.exp(carry_max + decay_total - new_max)
    new_scale = jnp.exp(block_max - new_max)
    new_memory = old_scale[:, None, None] * carry_memory + new_scale[:, None, None] * block_memory
    new_norm = old_scale[:, None] * carry_norm + new_scale[:, None] * block_norm
    return ((new_max, new_memory, new_norm), heads_out)

def reference(tokens, in_gain, w_query, w_key, w_value, w_input_gate, w_forget_gate, forget_bias, forget_extra, w_conv_gate, w_conv_left, w_conv_right, conv_taps, first_memory, first_norm, w_out_memory, w_out_conv):
    token_rows = tokens.astype(jnp.float32)
    scale_rows = lax.rsqrt(lax.optimization_barrier(jnp.mean(token_rows * token_rows, axis=1, keepdims=True)) + epsilon)
    normed = (token_rows * scale_rows * in_gain).astype(jnp.bfloat16)
    query_rows = jnp.dot(normed, w_query, preferred_element_type=jnp.float32).astype(jnp.bfloat16)
    key_rows = jnp.dot(normed, w_key, preferred_element_type=jnp.float32).astype(jnp.bfloat16)
    value_rows = jnp.dot(normed, w_value, preferred_element_type=jnp.float32).astype(jnp.bfloat16)
    in_pre = jnp.dot(normed, w_input_gate, preferred_element_type=jnp.float32)
    forget_pre = jnp.dot(normed, w_forget_gate, preferred_element_type=jnp.float32) + forget_bias
    log_forget = jax.nn.log_sigmoid(forget_pre) + forget_extra
    conv_gate = rounded(jnp.dot(normed, w_conv_gate, preferred_element_type=jnp.float32))
    conv_left = rounded(jnp.dot(normed, w_conv_left, preferred_element_type=jnp.float32))
    conv_right = rounded(jnp.dot(normed, w_conv_right, preferred_element_type=jnp.float32))
    product = (conv_left * conv_right).astype(jnp.bfloat16)
    padded = jnp.concatenate([jnp.zeros((TAPS - 1, CONV_CH), jnp.bfloat16), product], axis=0).astype(jnp.float32)
    filtered = conv_taps[0][None, :] * padded[0:SEQUENCE_TOKENS]
    for tap_index in range(1, TAPS):
        filtered = filtered + conv_taps[tap_index][None, :] * padded[tap_index:tap_index + SEQUENCE_TOKENS]
    conv_branch = (conv_gate * filtered).astype(jnp.bfloat16)
    blocks = SEQUENCE_TOKENS // TOK_DEV
    inputs = (query_rows.reshape(blocks, TOK_DEV, MEMORY_HEADS, KEY_DIM), key_rows.reshape(blocks, TOK_DEV, MEMORY_HEADS, KEY_DIM), value_rows.reshape(blocks, TOK_DEV, MEMORY_HEADS, VALUE_DIM), in_pre.reshape(blocks, TOK_DEV, MEMORY_HEADS), log_forget.reshape(blocks, TOK_DEV, MEMORY_HEADS))
    start_state = (jnp.zeros((MEMORY_HEADS,), jnp.float32), first_memory, first_norm)
    final_state, heads_out = lax.scan(mixer_block, start_state, inputs)
    heads_out = heads_out.reshape(SEQUENCE_TOKENS, V_WIDTH)
    head_group = V_WIDTH // N_TP
    channel_group = CONV_CH // N_TP
    mixed = jnp.zeros((SEQUENCE_TOKENS, D), jnp.float32)
    for group in range(N_TP):
        head_lo = group * head_group
        channel_lo = group * channel_group
        partial_value = jnp.dot(heads_out[:, head_lo:head_lo + head_group], w_out_memory[head_lo:head_lo + head_group], preferred_element_type=jnp.float32)
        partial_value = partial_value + jnp.dot(conv_branch[:, channel_lo:channel_lo + channel_group], w_out_conv[channel_lo:channel_lo + channel_group], preferred_element_type=jnp.float32)
        mixed = mixed + rounded(partial_value)
    return mixed.astype(jnp.bfloat16)
```

```python
import functools
import math

import jax
import jax.numpy as jnp
from jax import lax
from jax.experimental import pallas as pl
from jax.experimental.pallas import tpu as pltpu
from jax.sharding import PartitionSpec as P

KEY_DIM = 128
VALUE_DIM = 256
TAPS = 3
EPS = 1e-06
NEG = -1e30
MESH = pl.DeviceIdType.MESH
F32 = jnp.float32
BF16 = jnp.bfloat16
RS_CHUNKS = 8
PARTS = 4
MAX_SLOTS = 3


def mm(a, b):
    return lax.dot_general(a, b, (((1,), (0,)), ((), ())), preferred_element_type=F32)


def mm_t(a, b):
    return lax.dot_general(a, b, (((1,), (1,)), ((), ())), preferred_element_type=F32)


def scan_steps(n):
    steps, d = [], 1
    while d < n:
        steps.append(d)
        d *= 2
    return steps


def group_size(n_sp):
    b = 1
    while (2 * b) ** 2 <= n_sp and n_sp % (2 * b) == 0:
        b *= 2
    return b


def gather_pieces(rows):
    third = rows // 3
    return [(0, third), (third, third), (2 * third, third - 16), (rows - 16, 16)]


def kernel(
    n_sp, n_tp, heads, channels, width,
    tokens_h, gain_h, wk, wv, wq, wcg, wcl, wcr, wig_h, wfg_h, bias_h, extra_h, taps_h, first_mem_h, first_norm_h,
    wom, woc, out,
    TK, gain, wig, wfg, bias, extra, taps, first_mem, first_norm,
    W, WO, XG, PJ, G, RM, NUM, DEN, MO, CB, PROD, halo_out, halo_in,
    ST, SM, CO, CI, CSO, CSI, sq_out, sq_in, RC,
    PSC, PSM, DRC, DRM, YS, YR,
    i_sem, w_sem, ag_d, ag_ys, ag_yr, ag_fs, ag_fr, xs_s, xs_r, ch_s, ch_r, hl_s, sq_s, sq_r,
    cd_s, cd_r, rd_s, rd_r, ry_s, ry_r, ent,
):
    sp = lax.axis_index("sp")
    tp = lax.axis_index("tp")
    core = lax.rem(tp, 2)
    y = tp // 2
    n_y = n_tp // 2
    partner = tp + 1 - 2 * core
    R, D = TK.shape
    T = R * n_tp
    B = group_size(n_sp)
    A = n_sp // B
    zg, x_in = sp // B, lax.rem(sp, B)
    qk, vw = heads * KEY_DIM, heads * VALUE_DIM
    o_v, o_g = qk, qk + vw
    o_q = o_g + 128
    o_c = o_q + qk
    total = o_c + 3 * channels
    n_heads = wig.shape[0]

    def remote(src, dst, ss, rs, to_tp=None, to_sp=None):
        return pltpu.make_async_remote_copy(
            src_ref=src, dst_ref=dst, send_sem=ss, recv_sem=rs,
            device_id=(sp if to_sp is None else to_sp, tp if to_tp is None else to_tp),
            device_id_type=MESH,
        )

    barrier = pltpu.get_barrier_semaphore()
    for k in range(1, n_tp):
        pl.semaphore_signal(barrier, inc=1, device_id=(sp, lax.rem(tp + k, n_tp)), device_id_type=MESH)

    def later(fn):
        for k in range(1, B):
            pl.when(x_in + k < B)(functools.partial(fn, k))
        pl.when(zg < A - 1)(functools.partial(fn, B))
        if B > 1:
            pl.when((x_in == B - 1) & (zg < A - 1))(functools.partial(fn, 1))

    def earlier(fn):
        for k in range(1, B):
            pl.when(x_in >= k)(functools.partial(fn, k))
        pl.when(zg > 0)(functools.partial(fn, B))
        if B > 1:
            pl.when((x_in == 0) & (zg > 0))(functools.partial(fn, 1))

    extra_link = 1 if B > 1 else 0
    n_earlier = x_in + jnp.where(zg > 0, 1, 0) + extra_link * jnp.where((x_in == 0) & (zg > 0), 1, 0)
    n_later = (B - 1 - x_in + jnp.where(zg < A - 1, 1, 0)
               + extra_link * jnp.where((x_in == B - 1) & (zg < A - 1), 1, 0))
    later(lambda k: pl.semaphore_signal(barrier, inc=1, device_id=(sp + k, tp), device_id_type=MESH))

    inputs = [(tokens_h, TK), (gain_h, gain), (wig_h, wig), (wfg_h, wfg), (bias_h, bias), (extra_h, extra),
              (taps_h, taps), (first_mem_h, first_mem), (first_norm_h, first_norm)]
    in_copies = [pltpu.make_async_copy(s, d, i_sem.at[i]) for i, (s, d) in enumerate(inputs)]
    for c in in_copies[:4]:
        c.start()
    srcs = [(wk, 0, qk), (wv, o_v, vw), (wq, o_q, qk), (wcg, o_c, channels),
            (wcl, o_c + channels, channels), (wcr, o_c + 2 * channels, channels)]
    w_copies = [
        pltpu.make_async_copy(s, W.at[:, pl.ds(o, n)], w_sem.at[i])
        for i, (s, o, n) in enumerate(srcs)
    ]
    w_copies.append(pltpu.make_async_copy(woc, WO.at[pl.ds(vw, channels), :], w_sem.at[6]))
    w_copies.append(pltpu.make_async_copy(wom, WO.at[pl.ds(0, vw), :], w_sem.at[7]))
    for c in w_copies:
        c.start()
    for c in in_copies[4:]:
        c.start()

    def rows_of(block, first=0, n=None):
        n = R if n is None else n
        return pl.ds(pl.multiple_of(block * R + first, 16), n)

    def chip_rows(chip):
        return pl.ds(pl.multiple_of(chip * 2 * R, 16), 2 * R)

    in_copies[0].wait()
    in_copies[1].wait()
    x = TK[...].astype(F32)
    scale = lax.rsqrt(jnp.mean(x * x, axis=1, keepdims=True) + EPS)
    XG[rows_of(tp), :] = (x * scale * gain[...]).astype(BF16)
    pl.semaphore_wait(barrier, n_tp - 1 + n_earlier)
    earlier(lambda k: pl.semaphore_signal(ent, inc=1, device_id=(sp - k, tp), device_id_type=MESH))

    pieces = gather_pieces(R)
    third = R // 3
    sends = []

    def far_rows(chip, c, src_core):
        first, n = pieces[c]
        part = min(c, 2)
        at = chip * 2 * R + 2 * third * part + src_core * third + (first - part * third)
        return pl.ds(pl.multiple_of(at, 16), n)

    def y_piece(k, c, chip, to):
        src = XG.at[rows_of(tp, pieces[c][0], pieces[c][1]), :]
        return remote(src, XG.at[far_rows(chip, c, core), :], ag_ys.at[k - 1, c], ag_yr.at[k - 1, c], to_tp=to)

    for c in range(len(pieces)):
        for k in range(1, n_y):
            cp = y_piece(k, c, y, lax.rem(y + k, n_y) * 2 + core)
            cp.start()
            sends.append(cp)
    own = remote(XG.at[rows_of(tp), :], XG.at[rows_of(tp), :], ag_d.at[0], ag_d.at[1], to_tp=partner)
    own.start()

    def source(k):
        return lax.rem(y + n_y - k, n_y)

    def forward(c):
        for k in range(1, n_y):
            chip = source(k)
            y_piece(k, c, chip, partner).wait_recv()
            r = far_rows(chip, c, core)
            cp = remote(XG.at[r, :], XG.at[r, :], ag_fs.at[k - 1, c], ag_fr.at[k - 1, c], to_tp=partner)
            cp.start()
            sends.append(cp)

    def forwarded(c):
        for k in range(1, n_y):
            r = far_rows(source(k), c, 1 - core)
            remote(XG.at[r, :], XG.at[r, :], ag_fs.at[k - 1, c], ag_fr.at[k - 1, c], to_tp=partner).wait_recv()

    kv_cols = [(0, o_g)]
    rest_cols = [(o_q, qk)] + [(o_c + i * channels, channels) for i in range(3)]

    def project_local(cols):
        rr = chip_rows(y)
        for first, n in cols:
            PJ[rr, first:first + n] = mm(XG[rr, :], W[:, first:first + n]).astype(BF16)

    def local_gates():
        rr = chip_rows(y)
        G[rr, :] = mm(XG[rr, :], W[:, o_g:o_g + 128])

    def far_parts(part, chip):
        rr = pl.ds(pl.multiple_of(chip * 2 * R + 2 * third * part, 16), 2 * third)
        return rr, [rows_of(2 * chip + i, part * third, third) for i in range(2)]

    def project_far(part, cols):
        for k in range(1, n_y):
            rr, to = far_parts(part, source(k))
            for first, n in cols:
                res = mm(XG[rr, :], W[:, first:first + n]).astype(BF16)
                for i in range(2):
                    PJ[to[i], first:first + n] = res[i * third:(i + 1) * third]

    def far_gates(part):
        for k in range(1, n_y):
            rr, to = far_parts(part, source(k))
            res = mm(XG[rr, :], W[:, o_g:o_g + 128])
            for i in range(2):
                G[to[i], :] = res[i * third:(i + 1) * third]

    in_copies[2].wait()
    in_copies[3].wait()
    W[:, o_g:o_g + 128] = jnp.concatenate(
        [wig[...].astype(F32), wfg[...].astype(F32), jnp.zeros((128 - 2 * n_heads, D), F32)],
        axis=0).T.astype(BF16)
    for c in in_copies[4:]:
        c.wait()
    for c in w_copies[:2]:
        c.wait()
    own.wait_recv()
    project_local(kv_cols)
    local_gates()
    for c in w_copies[2:6]:
        c.wait()
    project_local(rest_cols)
    for part in range(2):
        forward(part)
        forwarded(part)
        project_far(part, kv_cols)
        far_gates(part)
        project_far(part, rest_cols)
    forward(2)
    forward(3)
    forwarded(2)
    forwarded(3)
    far_gates(2)
    project_far(2, kv_cols)

    gt = G[...].T
    in_all, forget_all = gt[0:n_heads], gt[n_heads:2 * n_heads]
    sub = lax.broadcasted_iota(jnp.int32, (n_heads, T), 0)
    sub8 = lax.broadcasted_iota(jnp.int32, (8, T), 0)
    lane = lax.broadcasted_iota(jnp.int32, (8, T), 1)
    in_pre = jnp.zeros((8, T), F32)
    log_f = jnp.zeros((8, T), F32)
    for h in range(heads):
        head = tp * heads + h
        row_i = jnp.sum(jnp.where(sub == head, in_all, 0.0), axis=0, keepdims=True)
        row_f = jnp.sum(jnp.where(sub == head, forget_all, 0.0), axis=0, keepdims=True) + bias[head]
        row_f = jnp.minimum(row_f, 0.0) - jnp.log1p(jnp.exp(-jnp.abs(row_f))) + extra[h:h + 1, :]
        in_pre = jnp.where(sub8 == h, row_i, in_pre)
        log_f = jnp.where(sub8 == h, row_f, log_f)
    cum = log_f
    for d in scan_steps(T):
        cum = cum + jnp.where(lane >= d, pltpu.roll(cum, d, 1), 0.0)
    gap = in_pre - cum
    decay = cum[:, T - 1:T]
    gmax = jnp.max(gap, axis=1, keepdims=True)
    w_all = jnp.exp(gap - gmax)
    w_hi = w_all.astype(BF16)
    w_lo = (w_all - w_hi.astype(F32)).astype(BF16)
    w_two = jnp.concatenate([w_hi, w_lo], axis=0)
    ones = jnp.ones((1, 128), F32)
    s8 = lax.broadcasted_iota(jnp.int32, (8, 128), 0)
    pr = KEY_DIM // PARTS

    def group_copies(k, h, p):
        to = sp - x_in + lax.rem(x_in + k, B)
        if p == 0:
            ref = SM.at[x_in, h]
        else:
            ref = ST.at[x_in, h, pl.ds((p - 1) * pr, pr), :]
        return remote(ref, ref, xs_s.at[k - 1, h, p], xs_r.at[k - 1, h, p], to_sp=to)

    def group_sends(fn):
        for k in range(1, B):
            pl.when((zg < A - 1) | (x_in + k < B))(functools.partial(fn, k))

    pl.when(sp < n_sp - 1)(lambda: pl.semaphore_wait(ent, n_later))
    for h in range(heads):
        k_t = PJ[:, h * KEY_DIM:(h + 1) * KEY_DIM].T
        keyed = (k_t.astype(F32) * w_all[h:h + 1, :]).astype(BF16)
        n2 = mm(w_two, PJ[:, h * KEY_DIM:(h + 1) * KEY_DIM])
        norm = n2[h:h + 1] + n2[8 + h:9 + h]
        d_row = decay[h:h + 1] * ones
        m_row = (decay[h:h + 1] + gmax[h:h + 1]) * ones
        SM[x_in, h] = jnp.where(s8 == 0, norm, jnp.where(s8 == 1, d_row, m_row))
        ST[x_in, h] = mm(keyed, PJ[:, o_v + h * VALUE_DIM:o_v + (h + 1) * VALUE_DIM]).astype(BF16)

        def go(k, h=h):
            for p in range(PARTS + 1):
                group_copies(k, h, p).start()

        group_sends(go)

    def weights(h, limit):
        valid = [j < limit for j in range(B)]
        ds = [jnp.where(valid[j], SM[j, h, 1:2], 0.0) for j in range(B)]
        ms = [jnp.where(valid[j], SM[j, h, 2:3], NEG) for j in range(B)]
        ns = [jnp.where(valid[j], SM[j, h, 0:1], 0.0) for j in range(B)]
        c_m = jnp.where(zg > 0, CSI[h, 2:3], 0.0)
        c_n = jnp.where(zg > 0, CSI[h, 0:1], first_norm[h:h + 1, :])
        after = [jnp.zeros((1, 128), F32)] * B
        for j in range(B - 2, -1, -1):
            after[j] = after[j + 1] + ds[j + 1]
        c_m = c_m + after[0] + ds[0]
        top = c_m
        for j in range(B):
            top = jnp.maximum(top, ms[j] + after[j])
        c_c = jnp.exp(c_m - top)
        c_j = [jnp.where(valid[j], jnp.exp(ms[j] + after[j] - top), 0.0) for j in range(B)]
        norm = c_c * c_n
        for j in range(B):
            norm = norm + c_j[j] * ns[j]
        return c_c, c_j, valid, norm, top

    def joined(h, wts, first, n):
        c_c, c_j, valid = wts[:3]
        two = lambda v: jnp.concatenate([v] * (VALUE_DIM // 128), axis=1)
        r = slice(first, first + n)
        mem = two(c_c) * jnp.where(zg > 0, CI[h, r].astype(F32), first_mem[h, r])
        for j in range(B):
            mem = mem + two(c_j[j]) * jnp.where(valid[j], ST[j, h, r].astype(F32), 0.0)
        return mem

    def chain_copy(h, p):
        if p == 0:
            s, d = CSO.at[h], CSI.at[h]
        else:
            rr = pl.ds((p - 1) * pr, pr)
            s, d = CO.at[h, rr, :], CI.at[h, rr, :]
        return remote(s, d, ch_s.at[h, p], ch_r.at[h, p], to_sp=sp + B)

    def chain_wait(h, p):
        if p == 0:
            d = CSI.at[h]
        else:
            d = CI.at[h, pl.ds((p - 1) * pr, pr), :]
        remote(d, d, ch_s.at[h, p], ch_r.at[h, p], to_tp=partner).wait_recv()

    def group_wait(k, h, p):
        j = lax.rem(x_in + B - k, B)
        d = SM.at[j, h] if p == 0 else ST.at[j, h, pl.ds((p - 1) * pr, pr), :]
        remote(d, d, xs_s.at[k - 1, h, p], xs_r.at[k - 1, h, p], to_tp=partner).wait_recv()

    def relay(chained):
        for h in range(heads):
            wts = None
            for p in range(PARTS + 1):
                for k in range(1, B):
                    group_wait(k, h, p)
                if chained:
                    chain_wait(h, p)
                if p == 0:
                    wts = weights(h, B)
                    CSO[h] = jnp.where(s8 == 0, wts[3], wts[4])
                else:
                    CO[h, (p - 1) * pr:p * pr] = joined(h, wts, (p - 1) * pr, pr).astype(BF16)
                chain_copy(h, p).start()

    def slot(s):
        last = min(MAX_SLOTS, A - 1)
        if s < last:
            pl.when(zg == s)(functools.partial(relay, s > 0))
        if s == last:
            if A - 1 > last:
                pl.when((zg >= last) & (zg < A - 1))(functools.partial(relay, True))

            @pl.when(zg == A - 1)
            def _():
                for h in range(heads):
                    for p in range(PARTS + 1):
                        for k in range(1, B):
                            pl.when(k <= x_in)(functools.partial(group_wait, k, h, p))
                        if A > 1:
                            chain_wait(h, p)

    rb = 256 if T % 256 == 0 else R
    q_scale = KEY_DIM ** -0.5
    shifted = gap + math.log(q_scale)

    def work_running_max():
        run = gap
        for d in scan_steps(T):
            run = jnp.maximum(run, jnp.where(lane >= d, pltpu.roll(run, d, 1), run))
        for h in range(heads):
            RM[h] = jnp.broadcast_to(run[h:h + 1], (128, T)).T

    def halo_copy(to):
        return remote(halo_out, halo_in, hl_s.at[0], hl_s.at[1], to_sp=to)

    def work_product():
        for r0 in range(0, T, rb):
            left = PJ[r0:r0 + rb, o_c + channels:o_c + 2 * channels].astype(F32)
            right = PJ[r0:r0 + rb, o_c + 2 * channels:o_c + 3 * channels].astype(F32)
            prod = (left * right).astype(BF16)
            PROD[8 + r0:8 + r0 + rb, :] = prod.astype(F32)
            if r0 + rb == T:
                halo_out[...] = prod[rb - 16:rb]
        pl.when(sp < n_sp - 1)(lambda: halo_copy(sp + 1).start())

    def attend(h, r0):
        e = r0 + rb
        q = PJ[r0:e, o_q + h * KEY_DIM:o_q + (h + 1) * KEY_DIM]
        k = PJ[0:e, h * KEY_DIM:(h + 1) * KEY_DIM]
        v = PJ[0:e, o_v + h * VALUE_DIM:o_v + (h + 1) * VALUE_DIM]
        s = mm_t(q, k)
        ti = lax.broadcasted_iota(jnp.int32, (rb, rb), 0)
        si = lax.broadcasted_iota(jnp.int32, (rb, rb), 1)
        rm = RM[h, r0:e, :]
        w = shifted[h:h + 1, 0:e] - jnp.concatenate([rm] * (e // 128), axis=1)
        diag = jnp.where(ti >= si, w[:, r0:e], NEG)
        w = jnp.concatenate([w[:, 0:r0], diag], axis=1) if r0 else diag
        mix = s * jnp.exp(w)
        DEN[h, r0:e, :] = jnp.broadcast_to(jnp.sum(mix, axis=1, keepdims=True), (rb, 128))
        NUM[r0:e, h * VALUE_DIM:(h + 1) * VALUE_DIM] = mm(mix.astype(BF16), v)

    def conv_finish():
        @pl.when(sp > 0)
        def _():
            halo_copy(sp).wait_recv()
            PROD[0:8, :] = halo_in[...].astype(F32)[8:16]

        @pl.when(sp == 0)
        def _():
            PROD[0:8, :] = jnp.zeros((8, channels), F32)

        tap = taps[:, pl.ds(pl.multiple_of(tp * channels, 128), channels)]
        for r0 in range(0, T, rb):
            f = tap[0:1] * PROD[6 + r0:6 + r0 + rb, :]
            f = f + tap[1:2] * PROD[7 + r0:7 + r0 + rb, :]
            f = f + tap[2:3] * PROD[8 + r0:8 + r0 + rb, :]
            gate = PJ[r0:r0 + rb, o_c:o_c + channels].astype(F32)
            CB[r0:r0 + rb, :] = (gate * f).astype(BF16)

    cw = D // RS_CHUNKS
    chips = [y] + [lax.rem(y + k, n_y) for k in range(1, n_y)]
    order = list(range(1, n_y)) + [0]

    def conv_copy(idx):
        return remote(PSC.at[rows_of(2 * chips[idx] + 1 - core), :], DRC.at[idx], cd_s.at[idx], cd_r.at[idx],
                      to_tp=partner)

    def conv_out():
        w_copies[6].wait()
        for idx in order:
            rr = chip_rows(chips[idx])
            for j in range(RS_CHUNKS):
                cols = slice(j * cw, (j + 1) * cw)
                PSC[rr, cols] = mm(CB[rr, :], WO[vw:, cols]).astype(BF16)
            conv_copy(idx).start()

    work_running_max()
    project_far(2, rest_cols)
    slot(0)
    work_product()
    for r0 in range(0, T, rb):
        attend(0, r0)
    slot(1)
    for h in range(1, heads):
        for r0 in range(0, T, rb):
            attend(h, r0)
    conv_finish()
    slot(2)
    conv_out()
    slot(3)

    sq = [None] * (T // rb)
    for h in range(heads):
        wts = weights(h, x_in)
        c_mem = joined(h, wts, 0, KEY_DIM)
        c_norm, cmax = wts[3], wts[4]
        hi = c_mem.astype(BF16)
        lo = (c_mem - hi.astype(F32)).astype(BF16)
        two = jnp.concatenate([hi, lo], axis=0)
        n_col = jnp.broadcast_to(c_norm, (128, 128)).T
        n_hi = n_col.astype(BF16)
        n_lo = (n_col - n_hi.astype(F32)).astype(BF16)
        n_two = jnp.concatenate([n_hi, n_lo], axis=0)
        for b, r0 in enumerate(range(0, T, rb)):
            e = r0 + rb
            q = PJ[r0:e, o_q + h * KEY_DIM:o_q + (h + 1) * KEY_DIM]
            qq = jnp.concatenate([q, q], axis=1)
            fm = mm(qq, two)
            fn = mm(qq, n_two)
            m0 = RM[h, r0:e, :]
            m = jnp.maximum(m0, cmax)
            k0 = jnp.exp(m0 - m)
            k1 = jnp.exp(cmax - m) * q_scale
            den = k0 * DEN[h, r0:e, :] + k1 * fn
            inv = 1.0 / jnp.maximum(jnp.abs(den), 1.0)
            k0, k1 = k0 * inv, k1 * inv
            cols = slice(h * VALUE_DIM, (h + 1) * VALUE_DIM)
            mo = (jnp.concatenate([k0, k0], axis=1) * NUM[r0:e, cols]
                  + jnp.concatenate([k1, k1], axis=1) * fm)
            MO[r0:e, cols] = mo.astype(BF16)
            s2 = mo * mo
            s2 = s2[:, 0:128] + s2[:, 128:256]
            sq[b] = s2 if sq[b] is None else sq[b] + s2
    sq_out[...] = jnp.zeros_like(sq_out)
    for b in range(T // rb):
        row = jnp.sum(sq[b].T, axis=0, keepdims=True)
        for i in range(rb // 128):
            at = b * (rb // 128) + i
            sq_out[at:at + 1, :] = row[:, i * 128:(i + 1) * 128]
    for k in range(1, n_tp):
        cp = remote(sq_out, sq_in.at[k - 1], sq_s.at[k - 1], sq_r.at[k - 1], to_tp=lax.rem(tp + k, n_tp))
        cp.start()
        sends.append(cp)

    def cols_of(j):
        return pl.ds(j * cw, cw)

    def mem_copy(idx, j):
        return remote(PSM.at[rows_of(2 * chips[idx] + 1 - core), cols_of(j)], DRM.at[idx, :, cols_of(j)],
                      rd_s.at[idx, j], rd_r.at[idx, j], to_tp=partner)

    w_copies[7].wait()
    for idx in order:
        rr = chip_rows(chips[idx])
        for j in range(RS_CHUNKS):
            cols = slice(j * cw, (j + 1) * cw)
            PSM[rr, cols] = mm(MO[rr, :], WO[0:vw, cols]).astype(BF16)
            mem_copy(idx, j).start()
    for idx in order:
        conv_copy(idx).wait_recv()

    tot = sq_out[...]
    for k in range(1, n_tp):
        remote(sq_out, sq_in.at[k - 1], sq_s.at[k - 1], sq_r.at[k - 1], to_tp=partner).wait_recv()
        tot = tot + sq_in[k - 1]
    r_scale = lax.rsqrt(tot / float(width) + EPS)
    for b in range(T // 128):
        RC[b * 128:(b + 1) * 128, :] = jnp.broadcast_to(r_scale[b:b + 1], (128, 128)).T

    def chip_sum(idx, j):
        cols = slice(j * cw, (j + 1) * cw)
        mine = rows_of(2 * chips[idx] + core)
        mem_copy(idx, j).wait_recv()
        r = jnp.concatenate([RC[mine, :]] * (cw // 128), axis=1)
        s = (PSM[mine, cols].astype(F32) + DRM[idx, :, cols].astype(F32)) * r
        return s + (PSC[mine, cols].astype(F32) + DRC[idx, :, cols].astype(F32))

    def y_copy(k, j):
        return remote(YS.at[k - 1, :, cols_of(j)], YR.at[k - 1, :, cols_of(j)], ry_s.at[k - 1, j],
                      ry_r.at[k - 1, j], to_tp=lax.rem(y + k, n_y) * 2 + core)

    for j in range(RS_CHUNKS):
        for k in range(1, n_y):
            YS[k - 1, :, j * cw:(j + 1) * cw] = chip_sum(k, j).astype(BF16)
            y_copy(k, j).start()
    for j in range(RS_CHUNKS):
        s = chip_sum(0, j)
        for k in range(1, n_y):
            y_copy(k, j).wait_recv()
            s = s + YR[k - 1, :, j * cw:(j + 1) * cw].astype(F32)
        out[:, j * cw:(j + 1) * cw] = s.astype(BF16)

    for cp in sends:
        cp.wait_send()
    own.wait_send()
    for h in range(heads):
        for p in range(PARTS + 1):
            group_sends(lambda k, h=h, p=p: group_copies(k, h, p).wait_send())

            @pl.when(zg < A - 1)
            def _(h=h, p=p):
                chain_copy(h, p).wait_send()
    pl.when(sp < n_sp - 1)(lambda: halo_copy(sp + 1).wait_send())
    for idx in range(n_y):
        conv_copy(idx).wait_send()
        for j in range(RS_CHUNKS):
            mem_copy(idx, j).wait_send()
    for k in range(1, n_y):
        for j in range(RS_CHUNKS):
            y_copy(k, j).wait_send()


def per_device(
    n_sp, n_tp,
    tokens, in_gain, w_query, w_key, w_value, w_input_gate, w_forget_gate, forget_bias,
    forget_extra, w_conv_gate, w_conv_left, w_conv_right, conv_taps, first_memory, first_norm,
    w_out_memory, w_out_conv,
):
    heads = w_query.shape[1] // KEY_DIM
    channels = w_conv_gate.shape[1]
    R, D = tokens.shape
    T = R * n_tp
    n_y = n_tp // 2
    qk, vw = heads * KEY_DIM, heads * VALUE_DIM
    total = 2 * qk + vw + 128 + 3 * channels
    n_heads = w_input_gate.shape[1]
    B = group_size(n_sp)
    hbm = pl.BlockSpec(memory_space=pl.ANY)
    V, dma = pltpu.VMEM, pltpu.SemaphoreType.DMA
    ny1 = n_y - 1
    np_ = len(gather_pieces(R))
    sq_rows = -(-T // 1024) * 8
    return pl.pallas_call(
        functools.partial(kernel, n_sp, n_tp, heads, channels, n_heads * VALUE_DIM),
        out_shape=pltpu.VMEM((R, D), BF16),
        in_specs=[hbm] * 17,
        out_specs=pl.BlockSpec(memory_space=pltpu.VMEM),
        scratch_shapes=[
            V((R, D), BF16), V((1, D), F32), V((n_heads, D), BF16), V((n_heads, D), BF16),
            pltpu.SMEM((n_heads,), F32), V((heads, T), F32), V((TAPS, n_tp * channels), F32),
            V((heads, KEY_DIM, VALUE_DIM), F32), V((heads, KEY_DIM), F32),
            V((D, total), BF16), V((vw + channels, D), BF16), V((T, D), BF16), V((T, total), BF16),
            V((T, 128), F32), V((heads, T, 128), F32), V((T, vw), F32), V((heads, T, 128), F32),
            V((T, vw), BF16), V((T, channels), BF16), V((8 + T, channels), F32),
            V((16, channels), BF16), V((16, channels), BF16),
            V((B, heads, KEY_DIM, VALUE_DIM), BF16), V((B, heads, 8, 128), F32),
            V((heads, KEY_DIM, VALUE_DIM), BF16), V((heads, KEY_DIM, VALUE_DIM), BF16),
            V((heads, 8, 128), F32), V((heads, 8, 128), F32),
            V((sq_rows, 128), F32), V((n_tp - 1, sq_rows, 128), F32), V((T, 128), F32),
            V((T, D), BF16), V((T, D), BF16), V((n_y, R, D), BF16), V((n_y, R, D), BF16),
            V((ny1, R, D), BF16), V((ny1, R, D), BF16),
            dma((9,)), dma((8,)), dma((2,)), dma((ny1, np_)), dma((ny1, np_)),
            dma((ny1, np_)), dma((ny1, np_)),
            dma((B - 1, heads, PARTS + 1)), dma((B - 1, heads, PARTS + 1)),
            dma((heads, PARTS + 1)), dma((heads, PARTS + 1)), dma((2,)),
            dma((n_tp - 1,)), dma((n_tp - 1,)), dma((n_y,)), dma((n_y,)),
            dma((n_y, RS_CHUNKS)), dma((n_y, RS_CHUNKS)), dma((ny1, RS_CHUNKS)), dma((ny1, RS_CHUNKS)),
            pltpu.SemaphoreType.REGULAR,
        ],
        compiler_params=pltpu.CompilerParams(
            collective_id=0, has_side_effects=True, vmem_limit_bytes=60 * 1024 * 1024),
        name="layer",
    )(
        tokens, in_gain.reshape(1, D), w_key, w_value, w_query, w_conv_gate, w_conv_left,
        w_conv_right, w_input_gate.T, w_forget_gate.T, forget_bias, forget_extra.T, conv_taps, first_memory, first_norm,
        w_out_memory, w_out_conv,
    )


def solution(mesh):
    in_specs = (
        P(("sp", "tp"), None), P(), P(None, "tp"), P(None, "tp"), P(None, "tp"), P(), P(), P(),
        P("sp", "tp"), P(None, "tp"), P(None, "tp"), P(None, "tp"), P(), P("tp", None, None),
        P("tp", None), P("tp", None), P("tp", None),
    )
    return jax.shard_map(
        functools.partial(per_device, mesh.shape["sp"], mesh.shape["tp"]),
        mesh=mesh, in_specs=in_specs, out_specs=P(("sp", "tp"), None), check_vma=False,
    )
```

```python
import functools
import math

import jax
import jax.numpy as jnp
from jax import lax
from jax.experimental import pallas as pl
from jax.experimental.pallas import tpu as pltpu
from jax.sharding import PartitionSpec as P

KEY_DIM = 128
VALUE_DIM = 256
TAPS = 3
EPS = 1e-06
NEG = -1e30
MESH = pl.DeviceIdType.MESH
F32 = jnp.float32
BF16 = jnp.bfloat16
RS_CHUNKS = 8
EARLY = 1
PARTS = 4
MAX_SLOTS = 3


def mm(a, b):
    return lax.dot_general(a, b, (((1,), (0,)), ((), ())), preferred_element_type=F32)


def mm_t(a, b):
    return lax.dot_general(a, b, (((1,), (1,)), ((), ())), preferred_element_type=F32)


def scan_steps(n):
    steps, d = [], 1
    while d < n:
        steps.append(d)
        d *= 2
    return steps


def group_size(n_sp):
    b = 1
    while (2 * b) ** 2 <= n_sp and n_sp % (2 * b) == 0:
        b *= 2
    return b


def gather_pieces(rows):
    third = rows // 3
    return [(0, third), (third, third), (2 * third, third - 16), (rows - 16, 16)]


def kernel(
    n_sp, n_tp, heads, channels, width,
    tokens_h, gain_h, wk, wv, wq, wcg, wcl, wcr, wig_h, wfg_h, bias_h, extra_h, taps_h, first_mem_h, first_norm_h,
    wom, woc, out,
    TK, gain, wig, wfg, bias, extra, taps, first_mem, first_norm,
    W, WO, XG, PJ, G, RM, NUM, DEN, MO, CB, PROD, halo_out, halo_in,
    ST, SM, CO, CI, CSO, CSI, sq_out, sq_in, RC,
    PSC, PSM, DRC, DRM, YS, YR, YC, YCR,
    i_sem, s_sem, ag_d, ag_yr, ag_fr, xs_r, ch_r, hl_r, sq_r, cd_r, rd_r, ry_r, yc_r, ent,
):
    sp = lax.axis_index("sp")
    tp = lax.axis_index("tp")
    core = lax.rem(tp, 2)
    y = tp // 2
    n_y = n_tp // 2
    partner = tp + 1 - 2 * core
    R, D = TK.shape
    T = R * n_tp
    B = group_size(n_sp)
    A = n_sp // B
    zg, x_in = sp // B, lax.rem(sp, B)
    qk, vw = heads * KEY_DIM, heads * VALUE_DIM
    o_v, o_g = qk, qk + vw
    o_q = o_g + 128
    o_c = o_q + qk
    total = o_c + 3 * channels
    n_heads = wig.shape[0]

    def remote(src, dst, ss, rs, to_tp=None, to_sp=None):
        return pltpu.make_async_remote_copy(
            src_ref=src, dst_ref=dst, send_sem=ss, recv_sem=rs,
            device_id=(sp if to_sp is None else to_sp, tp if to_tp is None else to_tp),
            device_id_type=MESH,
        )

    barrier = pltpu.get_barrier_semaphore()
    for k in range(1, n_tp):
        pl.semaphore_signal(barrier, inc=1, device_id=(sp, lax.rem(tp + k, n_tp)), device_id_type=MESH)

    def later(fn):
        for k in range(1, B):
            pl.when(x_in + k < B)(functools.partial(fn, k))
        pl.when(zg < A - 1)(functools.partial(fn, B))
        if B > 1:
            pl.when((x_in == B - 1) & (zg < A - 1))(functools.partial(fn, 1))

    def earlier(fn):
        for k in range(1, B):
            pl.when(x_in >= k)(functools.partial(fn, k))
        pl.when(zg > 0)(functools.partial(fn, B))
        if B > 1:
            pl.when((x_in == 0) & (zg > 0))(functools.partial(fn, 1))

    extra_link = 1 if B > 1 else 0
    n_earlier = x_in + jnp.where(zg > 0, 1, 0) + extra_link * jnp.where((x_in == 0) & (zg > 0), 1, 0)
    n_later = (B - 1 - x_in + jnp.where(zg < A - 1, 1, 0)
               + extra_link * jnp.where((x_in == B - 1) & (zg < A - 1), 1, 0))
    later(lambda k: pl.semaphore_signal(barrier, inc=1, device_id=(sp + k, tp), device_id_type=MESH))

    third = R // 3

    def copies(sem, pairs):
        return [pltpu.make_async_copy(a, b, i_sem.at[sem]) for a, b in pairs]

    token_copies = [copies(i, [(tokens_h.at[r, :], TK.at[r, :])])[0]
                    for i, r in enumerate([pl.ds(0, third), pl.ds(third, R - third)])]
    gate_copies = copies(2, [(gain_h, gain), (wig_h, wig), (wfg_h, wfg)])
    kv_copies = copies(3, [(wk, W.at[:, pl.ds(0, qk)]), (wv, W.at[:, pl.ds(o_v, vw)])])
    small_copies = copies(4, [(bias_h, bias), (extra_h, extra), (taps_h, taps),
                              (first_mem_h, first_mem), (first_norm_h, first_norm)])
    rest_copies = copies(5, [(wq, W.at[:, pl.ds(o_q, qk)])] + [
        (w, W.at[:, pl.ds(o_c + i * channels, channels)]) for i, w in enumerate((wcg, wcl, wcr))])
    out_copies = copies(6, [(woc, WO.at[pl.ds(vw, channels), :]), (wom, WO.at[pl.ds(0, vw), :])])
    for c in gate_copies + token_copies:
        c.start()

    def rows_of(block, first=0, n=None):
        n = R if n is None else n
        return pl.ds(pl.multiple_of(block * R + first, 16), n)

    def chip_rows(chip):
        return pl.ds(pl.multiple_of(chip * 2 * R, 16), 2 * R)

    pieces = gather_pieces(R)
    sends = []

    def far_rows(chip, c, src_core):
        first, n = pieces[c]
        part = min(c, 2)
        at = chip * 2 * R + 2 * third * part + src_core * third + (first - part * third)
        return pl.ds(pl.multiple_of(at, 16), n)

    def y_piece(k, c, chip, to):
        src = XG.at[rows_of(tp, pieces[c][0], pieces[c][1]), :]
        return remote(src, XG.at[far_rows(chip, c, core), :], s_sem, ag_yr.at[k - 1, c], to_tp=to)

    for c in gate_copies:
        c.wait()
    for c, (first, n) in enumerate(pieces):
        if c < 2:
            token_copies[c].wait()
        x = TK[first:first + n, :].astype(F32)
        scale = lax.rsqrt(jnp.mean(x * x, axis=1, keepdims=True) + EPS)
        XG[rows_of(tp, first, n), :] = (x * scale * gain[...]).astype(BF16)
        if c == 0:
            pl.semaphore_wait(barrier, n_tp - 1 + n_earlier)
        if c == 0 or c == len(pieces) - 1:
            for cc in [0] if c == 0 else range(1, len(pieces)):
                for k in range(1, n_y):
                    cp = y_piece(k, cc, y, lax.rem(y + k, n_y) * 2 + core)
                    cp.start()
                    sends.append(cp)
    for c in kv_copies + small_copies + rest_copies + out_copies:
        c.start()
    earlier(lambda k: pl.semaphore_signal(ent, inc=1, device_id=(sp - k, tp), device_id_type=MESH))
    own = remote(XG.at[rows_of(tp), :], XG.at[rows_of(tp), :], s_sem, ag_d, to_tp=partner)
    own.start()

    def source(k):
        return lax.rem(y + n_y - k, n_y)

    def forward(c):
        for k in range(1, n_y):
            chip = source(k)
            y_piece(k, c, chip, partner).wait_recv()
            r = far_rows(chip, c, core)
            cp = remote(XG.at[r, :], XG.at[r, :], s_sem, ag_fr.at[k - 1, c], to_tp=partner)
            cp.start()
            sends.append(cp)

    def forwarded(c):
        for k in range(1, n_y):
            r = far_rows(source(k), c, 1 - core)
            remote(XG.at[r, :], XG.at[r, :], s_sem, ag_fr.at[k - 1, c], to_tp=partner).wait_recv()

    kv_cols = [(0, o_g)]
    rest_cols = [(o_q, qk)] + [(o_c + i * channels, channels) for i in range(3)]

    def project_local(cols):
        rr = chip_rows(y)
        for first, n in cols:
            PJ[rr, first:first + n] = mm(XG[rr, :], W[:, first:first + n]).astype(BF16)

    def local_gates():
        rr = chip_rows(y)
        G[rr, :] = mm(XG[rr, :], W[:, o_g:o_g + 128])

    def far_parts(part, chip):
        rr = pl.ds(pl.multiple_of(chip * 2 * R + 2 * third * part, 16), 2 * third)
        return rr, [rows_of(2 * chip + i, part * third, third) for i in range(2)]

    def project_far(part, cols):
        for k in range(1, n_y):
            rr, to = far_parts(part, source(k))
            for first, n in cols:
                res = mm(XG[rr, :], W[:, first:first + n]).astype(BF16)
                for i in range(2):
                    PJ[to[i], first:first + n] = res[i * third:(i + 1) * third]

    def far_gates(part):
        for k in range(1, n_y):
            rr, to = far_parts(part, source(k))
            res = mm(XG[rr, :], W[:, o_g:o_g + 128])
            for i in range(2):
                G[to[i], :] = res[i * third:(i + 1) * third]

    W[:, o_g:o_g + 128] = jnp.concatenate(
        [wig[...].astype(F32), wfg[...].astype(F32), jnp.zeros((128 - 2 * n_heads, D), F32)],
        axis=0).T.astype(BF16)
    for c in kv_copies:
        c.wait()
    own.wait_recv()
    project_local(kv_cols)
    local_gates()
    for c in rest_copies:
        c.wait()
    project_local(rest_cols)
    for part in range(2):
        forward(part)
        forwarded(part)
        project_far(part, kv_cols)
        far_gates(part)
        project_far(part, rest_cols)
    forward(2)
    forward(3)
    forwarded(2)
    forwarded(3)
    for c in small_copies:
        c.wait()
    far_gates(2)

    gt = G[...].T
    in_all, forget_all = gt[0:n_heads], gt[n_heads:2 * n_heads]
    sub = lax.broadcasted_iota(jnp.int32, (n_heads, T), 0)
    sub8 = lax.broadcasted_iota(jnp.int32, (8, T), 0)
    lane = lax.broadcasted_iota(jnp.int32, (8, T), 1)
    in_pre = jnp.zeros((8, T), F32)
    log_f = jnp.zeros((8, T), F32)
    for h in range(heads):
        head = tp * heads + h
        row_i = jnp.sum(jnp.where(sub == head, in_all, 0.0), axis=0, keepdims=True)
        row_f = jnp.sum(jnp.where(sub == head, forget_all, 0.0), axis=0, keepdims=True) + bias[head]
        row_f = jnp.minimum(row_f, 0.0) - jnp.log1p(jnp.exp(-jnp.abs(row_f))) + extra[h:h + 1, :]
        in_pre = jnp.where(sub8 == h, row_i, in_pre)
        log_f = jnp.where(sub8 == h, row_f, log_f)
    cum = log_f
    for d in scan_steps(T):
        cum = cum + jnp.where(lane >= d, pltpu.roll(cum, d, 1), 0.0)
    gap = in_pre - cum
    decay = cum[:, T - 1:T]
    gmax = jnp.max(gap, axis=1, keepdims=True)
    w_all = jnp.exp(gap - gmax)
    w_hi = w_all.astype(BF16)
    w_lo = (w_all - w_hi.astype(F32)).astype(BF16)
    w_two = jnp.concatenate([w_hi, w_lo], axis=0)
    ones = jnp.ones((1, 128), F32)
    s8 = lax.broadcasted_iota(jnp.int32, (8, 128), 0)
    pr = KEY_DIM // PARTS

    project_far(2, kv_cols)

    def group_copies(k, h, p):
        to = sp - x_in + lax.rem(x_in + k, B)
        if p == 0:
            ref = SM.at[x_in, h]
        else:
            ref = ST.at[x_in, h, pl.ds((p - 1) * pr, pr), :]
        return remote(ref, ref, s_sem, xs_r.at[k - 1, h, p], to_sp=to)

    def group_sends(fn):
        for k in range(1, B):
            pl.when((zg < A - 1) | (x_in + k < B))(functools.partial(fn, k))

    pl.when(sp < n_sp - 1)(lambda: pl.semaphore_wait(ent, n_later))
    for h in range(heads):
        k_t = PJ[:, h * KEY_DIM:(h + 1) * KEY_DIM].T
        keyed = (k_t.astype(F32) * w_all[h:h + 1, :]).astype(BF16)
        n2 = mm(w_two, PJ[:, h * KEY_DIM:(h + 1) * KEY_DIM])
        norm = n2[h:h + 1] + n2[8 + h:9 + h]
        d_row = decay[h:h + 1] * ones
        m_row = (decay[h:h + 1] + gmax[h:h + 1]) * ones
        SM[x_in, h] = jnp.where(s8 == 0, norm, jnp.where(s8 == 1, d_row, m_row))
        ST[x_in, h] = mm(keyed, PJ[:, o_v + h * VALUE_DIM:o_v + (h + 1) * VALUE_DIM]).astype(BF16)

        def go(k, h=h):
            for p in range(PARTS + 1):
                group_copies(k, h, p).start()

        group_sends(go)

    def weights(h, limit):
        valid = [j < limit for j in range(B)]
        ds = [jnp.where(valid[j], SM[j, h, 1:2], 0.0) for j in range(B)]
        ms = [jnp.where(valid[j], SM[j, h, 2:3], NEG) for j in range(B)]
        ns = [jnp.where(valid[j], SM[j, h, 0:1], 0.0) for j in range(B)]
        c_m = jnp.where(zg > 0, CSI[h, 2:3], 0.0)
        c_n = jnp.where(zg > 0, CSI[h, 0:1], first_norm[h:h + 1, :])
        after = [jnp.zeros((1, 128), F32)] * B
        for j in range(B - 2, -1, -1):
            after[j] = after[j + 1] + ds[j + 1]
        c_m = c_m + after[0] + ds[0]
        top = c_m
        for j in range(B):
            top = jnp.maximum(top, ms[j] + after[j])
        c_c = jnp.exp(c_m - top)
        c_j = [jnp.where(valid[j], jnp.exp(ms[j] + after[j] - top), 0.0) for j in range(B)]
        norm = c_c * c_n
        for j in range(B):
            norm = norm + c_j[j] * ns[j]
        return c_c, c_j, valid, norm, top

    def joined(h, wts, first, n):
        c_c, c_j, valid = wts[:3]
        two = lambda v: jnp.concatenate([v] * (VALUE_DIM // 128), axis=1)
        r = slice(first, first + n)
        mem = two(c_c) * jnp.where(zg > 0, CI[h, r].astype(F32), first_mem[h, r])
        for j in range(B):
            mem = mem + two(c_j[j]) * jnp.where(valid[j], ST[j, h, r].astype(F32), 0.0)
        return mem

    def chain_copy(h, p):
        if p == 0:
            s, d = CSO.at[h], CSI.at[h]
        else:
            rr = pl.ds((p - 1) * pr, pr)
            s, d = CO.at[h, rr, :], CI.at[h, rr, :]
        return remote(s, d, s_sem, ch_r.at[h, p], to_sp=sp + B)

    def chain_wait(h, p):
        if p == 0:
            d = CSI.at[h]
        else:
            d = CI.at[h, pl.ds((p - 1) * pr, pr), :]
        remote(d, d, s_sem, ch_r.at[h, p], to_tp=partner).wait_recv()

    def group_wait(k, h, p):
        j = lax.rem(x_in + B - k, B)
        d = SM.at[j, h] if p == 0 else ST.at[j, h, pl.ds((p - 1) * pr, pr), :]
        remote(d, d, s_sem, xs_r.at[k - 1, h, p], to_tp=partner).wait_recv()

    def relay(chained):
        for h in range(heads):
            wts = None
            for p in range(PARTS + 1):
                for k in range(1, B):
                    group_wait(k, h, p)
                if chained:
                    chain_wait(h, p)
                if p == 0:
                    wts = weights(h, B)
                    CSO[h] = jnp.where(s8 == 0, wts[3], wts[4])
                else:
                    CO[h, (p - 1) * pr:p * pr] = joined(h, wts, (p - 1) * pr, pr).astype(BF16)
                chain_copy(h, p).start()

    def slot(s):
        last = min(MAX_SLOTS, A - 1)
        if s < last:
            pl.when(zg == s)(functools.partial(relay, s > 0))
        if s == last and A - 1 > last:
            pl.when((zg >= last) & (zg < A - 1))(functools.partial(relay, True))

    def end_wait(h):
        @pl.when(zg == A - 1)
        def _():
            for p in range(PARTS + 1):
                for k in range(1, B):
                    pl.when(k <= x_in)(functools.partial(group_wait, k, h, p))
                if A > 1:
                    chain_wait(h, p)

    rb = 256 if T % 256 == 0 else R
    q_scale = KEY_DIM ** -0.5
    shifted = gap + math.log(q_scale)

    def work_running_max():
        run = gap
        for d in scan_steps(T):
            run = jnp.maximum(run, jnp.where(lane >= d, pltpu.roll(run, d, 1), run))
        for h in range(heads):
            RM[h] = jnp.broadcast_to(run[h:h + 1], (128, T)).T

    def halo_copy(to):
        return remote(halo_out, halo_in, s_sem, hl_r, to_sp=to)

    def work_product():
        for r0 in range(0, T, rb):
            left = PJ[r0:r0 + rb, o_c + channels:o_c + 2 * channels].astype(F32)
            right = PJ[r0:r0 + rb, o_c + 2 * channels:o_c + 3 * channels].astype(F32)
            prod = (left * right).astype(BF16)
            PROD[8 + r0:8 + r0 + rb, :] = prod.astype(F32)
            if r0 + rb == T:
                halo_out[...] = prod[rb - 16:rb]
        pl.when(sp < n_sp - 1)(lambda: halo_copy(sp + 1).start())

    def attend(h, r0):
        e = r0 + rb
        q = PJ[r0:e, o_q + h * KEY_DIM:o_q + (h + 1) * KEY_DIM]
        k = PJ[0:e, h * KEY_DIM:(h + 1) * KEY_DIM]
        v = PJ[0:e, o_v + h * VALUE_DIM:o_v + (h + 1) * VALUE_DIM]
        s = mm_t(q, k)
        ti = lax.broadcasted_iota(jnp.int32, (rb, rb), 0)
        si = lax.broadcasted_iota(jnp.int32, (rb, rb), 1)
        rm = RM[h, r0:e, :]
        w = shifted[h:h + 1, 0:e] - jnp.concatenate([rm] * (e // 128), axis=1)
        diag = jnp.where(ti >= si, w[:, r0:e], NEG)
        w = jnp.concatenate([w[:, 0:r0], diag], axis=1) if r0 else diag
        mix = s * jnp.exp(w)
        DEN[h, r0:e, :] = jnp.broadcast_to(jnp.sum(mix, axis=1, keepdims=True), (rb, 128))
        NUM[r0:e, h * VALUE_DIM:(h + 1) * VALUE_DIM] = mm(mix.astype(BF16), v)

    def conv_finish():
        @pl.when(sp > 0)
        def _():
            halo_copy(sp).wait_recv()
            PROD[0:8, :] = halo_in[...].astype(F32)[8:16]

        @pl.when(sp == 0)
        def _():
            PROD[0:8, :] = jnp.zeros((8, channels), F32)

        tap = taps[:, pl.ds(pl.multiple_of(tp * channels, 128), channels)]
        for r0 in range(0, T, rb):
            f = tap[0:1] * PROD[6 + r0:6 + r0 + rb, :]
            f = f + tap[1:2] * PROD[7 + r0:7 + r0 + rb, :]
            f = f + tap[2:3] * PROD[8 + r0:8 + r0 + rb, :]
            gate = PJ[r0:r0 + rb, o_c:o_c + channels].astype(F32)
            CB[r0:r0 + rb, :] = (gate * f).astype(BF16)

    cw = D // RS_CHUNKS
    chips = [y] + [lax.rem(y + k, n_y) for k in range(1, n_y)]
    order = list(range(1, n_y)) + [0]

    def conv_copy(idx):
        return remote(PSC.at[rows_of(2 * chips[idx] + 1 - core), :], DRC.at[idx], s_sem, cd_r.at[idx],
                      to_tp=partner)

    def conv_out(which):
        for idx in which:
            rr = chip_rows(chips[idx])
            for j in range(RS_CHUNKS):
                cols = slice(j * cw, (j + 1) * cw)
                PSC[rr, cols] = mm(CB[rr, :], WO[vw:, cols]).astype(BF16)
            conv_copy(idx).start()

    early = EARLY * cw

    def early_copy(k):
        return remote(YC.at[k - 1], YCR.at[k - 1], s_sem, yc_r.at[k - 1],
                      to_tp=lax.rem(y + k, n_y) * 2 + core)

    def conv_early():
        for k in range(1, n_y):
            conv_copy(k).wait_recv()
            mine = rows_of(2 * chips[k] + core)
            s = PSC[mine, 0:early].astype(F32) + DRC[k, :, 0:early].astype(F32)
            YC[k - 1] = s.astype(BF16)
            early_copy(k).start()

    work_running_max()
    project_far(2, rest_cols)
    work_product()
    for h in range(heads):
        for r0 in range(0, T, rb):
            attend(h, r0)
    slot(0)
    slot(1)
    conv_finish()
    for c in out_copies:
        c.wait()
    conv_out(order[:-1])
    slot(2)
    conv_out(order[-1:])
    conv_early()
    slot(3)

    sq = [None] * (T // rb)
    for h in range(heads):
        end_wait(h)
        wts = weights(h, x_in)
        c_mem = joined(h, wts, 0, KEY_DIM)
        c_norm, cmax = wts[3], wts[4]
        hi = c_mem.astype(BF16)
        lo = (c_mem - hi.astype(F32)).astype(BF16)
        two = jnp.concatenate([hi, lo], axis=0)
        n_col = jnp.broadcast_to(c_norm, (128, 128)).T
        n_hi = n_col.astype(BF16)
        n_lo = (n_col - n_hi.astype(F32)).astype(BF16)
        n_two = jnp.concatenate([n_hi, n_lo], axis=0)
        for b, r0 in enumerate(range(0, T, rb)):
            e = r0 + rb
            q = PJ[r0:e, o_q + h * KEY_DIM:o_q + (h + 1) * KEY_DIM]
            qq = jnp.concatenate([q, q], axis=1)
            fm = mm(qq, two)
            fn = mm(qq, n_two)
            m0 = RM[h, r0:e, :]
            m = jnp.maximum(m0, cmax)
            k0 = jnp.exp(m0 - m)
            k1 = jnp.exp(cmax - m) * q_scale
            den = k0 * DEN[h, r0:e, :] + k1 * fn
            inv = 1.0 / jnp.maximum(jnp.abs(den), 1.0)
            k0, k1 = k0 * inv, k1 * inv
            cols = slice(h * VALUE_DIM, (h + 1) * VALUE_DIM)
            mo = (jnp.concatenate([k0, k0], axis=1) * NUM[r0:e, cols]
                  + jnp.concatenate([k1, k1], axis=1) * fm)
            MO[r0:e, cols] = mo.astype(BF16)
            s2 = mo * mo
            s2 = s2[:, 0:128] + s2[:, 128:256]
            sq[b] = s2 if sq[b] is None else sq[b] + s2
    sq_out[...] = jnp.zeros_like(sq_out)
    for b in range(T // rb):
        row = jnp.sum(sq[b].T, axis=0, keepdims=True)
        for i in range(rb // 128):
            at = b * (rb // 128) + i
            sq_out[at:at + 1, :] = row[:, i * 128:(i + 1) * 128]
    for k in range(1, n_tp):
        cp = remote(sq_out, sq_in.at[k - 1], s_sem, sq_r, to_tp=lax.rem(tp + k, n_tp))
        cp.start()
        sends.append(cp)

    def cols_of(j):
        return pl.ds(j * cw, cw)

    parts = [(0, EARLY), (EARLY, RS_CHUNKS)]

    def mem_copy(idx, q):
        cols = pl.ds(parts[q][0] * cw, (parts[q][1] - parts[q][0]) * cw)
        return remote(PSM.at[rows_of(2 * chips[idx] + 1 - core), cols], DRM.at[idx, :, cols],
                      s_sem, rd_r.at[idx, q], to_tp=partner)

    def mem_out(idx):
        rr = chip_rows(chips[idx])
        for q in range(2):
            for j in range(*parts[q]):
                cols = slice(j * cw, (j + 1) * cw)
                PSM[rr, cols] = mm(MO[rr, :], WO[0:vw, cols]).astype(BF16)
            mem_copy(idx, q).start()

    def y_copy(k, j):
        return remote(YS.at[k - 1, :, cols_of(j)], YR.at[k - 1, :, cols_of(j)], s_sem,
                      ry_r.at[k - 1, j], to_tp=lax.rem(y + k, n_y) * 2 + core)

    def mem_sum(idx, j):
        cols = slice(j * cw, (j + 1) * cw)
        mine = rows_of(2 * chips[idx] + core)
        return PSM[mine, cols].astype(F32) + DRM[idx, :, cols].astype(F32)

    for idx in order[:-1]:
        mem_out(idx)
    for k in range(1, n_y):
        mem_copy(k, 0).wait_recv()
        for j in range(EARLY):
            YS[k - 1, :, j * cw:(j + 1) * cw] = mem_sum(k, j).astype(BF16)
            y_copy(k, j).start()
    mem_out(0)

    tot = sq_out[...]
    remote(sq_in, sq_in, s_sem, sq_r, to_tp=partner).wait_recv()
    for k in range(1, n_tp):
        tot = tot + sq_in[k - 1]
    r_scale = lax.rsqrt(tot / float(width) + EPS)
    for b in range(T // 128):
        RC[b * 128:(b + 1) * 128, :] = jnp.broadcast_to(r_scale[b:b + 1], (128, 128)).T

    def row_scale(idx):
        return jnp.concatenate([RC[rows_of(2 * chips[idx] + core), :]] * (cw // 128), axis=1)

    def chip_sum(idx, j):
        cols = slice(j * cw, (j + 1) * cw)
        mine = rows_of(2 * chips[idx] + core)
        s = PSC[mine, cols].astype(F32) + DRC[idx, :, cols].astype(F32)
        return s + mem_sum(idx, j) * row_scale(idx)

    for k in range(1, n_y):
        mem_copy(k, 1).wait_recv()
        for j in range(EARLY, RS_CHUNKS):
            YS[k - 1, :, j * cw:(j + 1) * cw] = chip_sum(k, j).astype(BF16)
            y_copy(k, j).start()
    conv_copy(0).wait_recv()
    for q in range(2):
        mem_copy(0, q).wait_recv()
    for k in range(1, n_y):
        early_copy(k).wait_recv()
    for j in range(RS_CHUNKS):
        s = chip_sum(0, j)
        for k in range(1, n_y):
            y_copy(k, j).wait_recv()
            got = YR[k - 1, :, j * cw:(j + 1) * cw].astype(F32)
            if j < EARLY:
                got = got * row_scale(0) + YCR[k - 1, :, j * cw:(j + 1) * cw].astype(F32)
            s = s + got
        out[:, j * cw:(j + 1) * cw] = s.astype(BF16)

    for cp in sends:
        cp.wait_send()
    own.wait_send()
    for h in range(heads):
        for p in range(PARTS + 1):
            group_sends(lambda k, h=h, p=p: group_copies(k, h, p).wait_send())

            @pl.when(zg < A - 1)
            def _(h=h, p=p):
                chain_copy(h, p).wait_send()
    pl.when(sp < n_sp - 1)(lambda: halo_copy(sp + 1).wait_send())
    for idx in range(n_y):
        conv_copy(idx).wait_send()
        for q in range(2):
            mem_copy(idx, q).wait_send()
    for k in range(1, n_y):
        early_copy(k).wait_send()
        for j in range(RS_CHUNKS):
            y_copy(k, j).wait_send()


def per_device(
    n_sp, n_tp,
    tokens, in_gain, w_query, w_key, w_value, w_input_gate, w_forget_gate, forget_bias,
    forget_extra, w_conv_gate, w_conv_left, w_conv_right, conv_taps, first_memory, first_norm,
    w_out_memory, w_out_conv,
):
    heads = w_query.shape[1] // KEY_DIM
    channels = w_conv_gate.shape[1]
    R, D = tokens.shape
    T = R * n_tp
    n_y = n_tp // 2
    qk, vw = heads * KEY_DIM, heads * VALUE_DIM
    total = 2 * qk + vw + 128 + 3 * channels
    n_heads = w_input_gate.shape[1]
    B = group_size(n_sp)
    hbm = pl.BlockSpec(memory_space=pl.ANY)
    V, dma = pltpu.VMEM, pltpu.SemaphoreType.DMA
    ny1 = n_y - 1
    np_ = len(gather_pieces(R))
    sq_rows = -(-T // 1024) * 8
    early = EARLY * D // RS_CHUNKS
    return pl.pallas_call(
        functools.partial(kernel, n_sp, n_tp, heads, channels, n_heads * VALUE_DIM),
        out_shape=pltpu.VMEM((R, D), BF16),
        in_specs=[hbm] * 17,
        out_specs=pl.BlockSpec(memory_space=pltpu.VMEM),
        scratch_shapes=[
            V((R, D), BF16), V((1, D), F32), V((n_heads, D), BF16), V((n_heads, D), BF16),
            pltpu.SMEM((n_heads,), F32), V((heads, T), F32), V((TAPS, n_tp * channels), F32),
            V((heads, KEY_DIM, VALUE_DIM), F32), V((heads, KEY_DIM), F32),
            V((D, total), BF16), V((vw + channels, D), BF16), V((T, D), BF16), V((T, total), BF16),
            V((T, 128), F32), V((heads, T, 128), F32), V((T, vw), F32), V((heads, T, 128), F32),
            V((T, vw), BF16), V((T, channels), BF16), V((8 + T, channels), F32),
            V((16, channels), BF16), V((16, channels), BF16),
            V((B, heads, KEY_DIM, VALUE_DIM), BF16), V((B, heads, 8, 128), F32),
            V((heads, KEY_DIM, VALUE_DIM), BF16), V((heads, KEY_DIM, VALUE_DIM), BF16),
            V((heads, 8, 128), F32), V((heads, 8, 128), F32),
            V((sq_rows, 128), F32), V((n_tp - 1, sq_rows, 128), F32), V((T, 128), F32),
            V((T, D), BF16), V((T, D), BF16), V((n_y, R, D), BF16), V((n_y, R, D), BF16),
            V((ny1, R, D), BF16), V((ny1, R, D), BF16),
            V((ny1, R, early), BF16), V((ny1, R, early), BF16),
            dma((7,)), dma, dma, dma((ny1, np_)), dma((ny1, np_)), dma((B - 1, heads, PARTS + 1)),
            dma((heads, PARTS + 1)), dma, dma, dma((n_y,)), dma((n_y, 2)), dma((ny1, RS_CHUNKS)), dma((ny1,)),
            pltpu.SemaphoreType.REGULAR,
        ],
        compiler_params=pltpu.CompilerParams(
            collective_id=0, has_side_effects=True, vmem_limit_bytes=60 * 1024 * 1024),
        name="layer",
    )(
        tokens, in_gain.reshape(1, D), w_key, w_value, w_query, w_conv_gate, w_conv_left,
        w_conv_right, w_input_gate.T, w_forget_gate.T, forget_bias, forget_extra.T, conv_taps, first_memory, first_norm,
        w_out_memory, w_out_conv,
    )


def solution(mesh):
    in_specs = (
        P(("sp", "tp"), None), P(), P(None, "tp"), P(None, "tp"), P(None, "tp"), P(), P(), P(),
        P("sp", "tp"), P(None, "tp"), P(None, "tp"), P(None, "tp"), P(), P("tp", None, None),
        P("tp", None), P("tp", None), P("tp", None),
    )
    return jax.shard_map(
        functools.partial(per_device, mesh.shape["sp"], mesh.shape["tp"]),
        mesh=mesh, in_specs=in_specs, out_specs=P(("sp", "tp"), None), check_vma=False,
    )
```

```python
import functools
import math

import jax
import jax.numpy as jnp
from jax import lax
from jax.experimental import pallas as pl
from jax.experimental.pallas import tpu as pltpu
from jax.sharding import PartitionSpec as P

KEY_DIM = 128
VALUE_DIM = 256
TAPS = 3
EPS = 1e-06
NEG = -1e30
MESH = pl.DeviceIdType.MESH
F32 = jnp.float32
BF16 = jnp.bfloat16
RS_CHUNKS = 8
EARLY = 1
PARTS = 4
MAX_SLOTS = 3


def mm(a, b):
    return lax.dot_general(a, b, (((1,), (0,)), ((), ())), preferred_element_type=F32)


def mm_t(a, b):
    return lax.dot_general(a, b, (((1,), (1,)), ((), ())), preferred_element_type=F32)


def scan_steps(n):
    steps, d = [], 1
    while d < n:
        steps.append(d)
        d *= 2
    return steps


def group_size(n_sp):
    b = 1
    while (2 * b) ** 2 <= n_sp and n_sp % (2 * b) == 0:
        b *= 2
    return b


def gather_pieces(rows):
    third = rows // 3
    return [(0, third), (third, third), (2 * third, third - 16), (rows - 16, 16)]


def kernel(
    n_sp, n_tp, heads, channels, width,
    tokens_h, gain_h, wk, wv, wq, wcg, wcl, wcr, wig_h, wfg_h, bias_h, extra_h, taps_h, first_mem_h, first_norm_h,
    wom, woc, out,
    TK, gain, wig, wfg, bias, extra, taps, first_mem, first_norm,
    W, WO, XG, PJ, G, RM, NUM, DEN, MO, CB, PROD, halo_out, halo_in,
    ST, SM, CO, CI, CSO, CSI, CW, sq_out, sq_in, RC,
    PSC, PSM, DRC, DRM, YS, YR, YC, YCR,
    i_sem, s_sem, ag_d, ag_yr, ag_fr, xs_r, ch_r, hl_r, sq_r, cd_r, rd_r, ry_r, yc_r, ent,
):
    sp = lax.axis_index("sp")
    tp = lax.axis_index("tp")
    core = lax.rem(tp, 2)
    y = tp // 2
    n_y = n_tp // 2
    partner = tp + 1 - 2 * core
    R, D = TK.shape
    T = R * n_tp
    B = group_size(n_sp)
    A = n_sp // B
    zg, x_in = sp // B, lax.rem(sp, B)
    qk, vw = heads * KEY_DIM, heads * VALUE_DIM
    o_v, o_g = qk, qk + vw
    o_q = o_g + 128
    o_c = o_q + qk
    total = o_c + 3 * channels
    n_heads = wig.shape[0]

    def remote(src, dst, ss, rs, to_tp=None, to_sp=None):
        return pltpu.make_async_remote_copy(
            src_ref=src, dst_ref=dst, send_sem=ss, recv_sem=rs,
            device_id=(sp if to_sp is None else to_sp, tp if to_tp is None else to_tp),
            device_id_type=MESH,
        )

    barrier = pltpu.get_barrier_semaphore()
    for k in range(1, n_tp):
        pl.semaphore_signal(barrier, inc=1, device_id=(sp, lax.rem(tp + k, n_tp)), device_id_type=MESH)

    def later(fn):
        for k in range(1, B):
            pl.when(x_in + k < B)(functools.partial(fn, k))
        pl.when(zg < A - 1)(functools.partial(fn, B))
        if B > 1:
            pl.when((x_in == B - 1) & (zg < A - 1))(functools.partial(fn, 1))

    def earlier(fn):
        for k in range(1, B):
            pl.when(x_in >= k)(functools.partial(fn, k))
        pl.when(zg > 0)(functools.partial(fn, B))
        if B > 1:
            pl.when((x_in == 0) & (zg > 0))(functools.partial(fn, 1))

    extra_link = 1 if B > 1 else 0
    n_earlier = x_in + jnp.where(zg > 0, 1, 0) + extra_link * jnp.where((x_in == 0) & (zg > 0), 1, 0)
    n_later = (B - 1 - x_in + jnp.where(zg < A - 1, 1, 0)
               + extra_link * jnp.where((x_in == B - 1) & (zg < A - 1), 1, 0))
    later(lambda k: pl.semaphore_signal(barrier, inc=1, device_id=(sp + k, tp), device_id_type=MESH))

    third = R // 3

    def copies(sem, pairs):
        return [pltpu.make_async_copy(a, b, i_sem.at[sem]) for a, b in pairs]

    token_copies = [copies(i, [(tokens_h.at[r, :], TK.at[r, :])])[0]
                    for i, r in enumerate([pl.ds(0, third), pl.ds(third, R - third)])]
    gate_copies = copies(2, [(gain_h, gain), (wig_h, wig), (wfg_h, wfg)])
    kv_copies = copies(3, [(wk, W.at[:, pl.ds(0, qk)]), (wv, W.at[:, pl.ds(o_v, vw)])])
    small_copies = copies(4, [(bias_h, bias), (extra_h, extra), (taps_h, taps),
                              (first_mem_h, first_mem), (first_norm_h, first_norm)])
    rest_copies = copies(5, [(wq, W.at[:, pl.ds(o_q, qk)])] + [
        (w, W.at[:, pl.ds(o_c + i * channels, channels)]) for i, w in enumerate((wcg, wcl, wcr))])
    out_copies = copies(6, [(woc, WO.at[pl.ds(vw, channels), :]), (wom, WO.at[pl.ds(0, vw), :])])
    for c in token_copies[:1] + gate_copies + token_copies[1:]:
        c.start()

    def rows_of(block, first=0, n=None):
        n = R if n is None else n
        return pl.ds(pl.multiple_of(block * R + first, 16), n)

    def chip_rows(chip):
        return pl.ds(pl.multiple_of(chip * 2 * R, 16), 2 * R)

    pieces = gather_pieces(R)
    sends = []

    def far_rows(chip, c, src_core):
        first, n = pieces[c]
        part = min(c, 2)
        at = chip * 2 * R + 2 * third * part + src_core * third + (first - part * third)
        return pl.ds(pl.multiple_of(at, 16), n)

    def y_piece(k, c, chip, to):
        src = XG.at[rows_of(tp, pieces[c][0], pieces[c][1]), :]
        return remote(src, XG.at[far_rows(chip, c, core), :], s_sem, ag_yr.at[k - 1, c], to_tp=to)

    for c in gate_copies:
        c.wait()
    for c, (first, n) in enumerate(pieces):
        if c < 2:
            token_copies[c].wait()
        x = TK[first:first + n, :].astype(F32)
        scale = lax.rsqrt(jnp.mean(x * x, axis=1, keepdims=True) + EPS)
        XG[rows_of(tp, first, n), :] = (x * scale * gain[...]).astype(BF16)
        if c == 0:
            pl.semaphore_wait(barrier, n_tp - 1 + n_earlier)
        if c == 0 or c == len(pieces) - 1:
            for cc in [0] if c == 0 else range(1, len(pieces)):
                for k in range(1, n_y):
                    cp = y_piece(k, cc, y, lax.rem(y + k, n_y) * 2 + core)
                    cp.start()
                    sends.append(cp)
    for c in kv_copies + small_copies + rest_copies + out_copies:
        c.start()
    earlier(lambda k: pl.semaphore_signal(ent, inc=1, device_id=(sp - k, tp), device_id_type=MESH))
    own = remote(XG.at[rows_of(tp), :], XG.at[rows_of(tp), :], s_sem, ag_d, to_tp=partner)
    own.start()

    def source(k):
        return lax.rem(y + n_y - k, n_y)

    def forward(c):
        for k in range(1, n_y):
            chip = source(k)
            y_piece(k, c, chip, partner).wait_recv()
            r = far_rows(chip, c, core)
            cp = remote(XG.at[r, :], XG.at[r, :], s_sem, ag_fr.at[k - 1, c], to_tp=partner)
            cp.start()
            sends.append(cp)

    def forwarded(c):
        for k in range(1, n_y):
            r = far_rows(source(k), c, 1 - core)
            remote(XG.at[r, :], XG.at[r, :], s_sem, ag_fr.at[k - 1, c], to_tp=partner).wait_recv()

    kv_cols = [(0, o_g)]
    rest_cols = [(o_q, qk)] + [(o_c + i * channels, channels) for i in range(3)]

    def project_local(cols):
        rr = chip_rows(y)
        for first, n in cols:
            PJ[rr, first:first + n] = mm(XG[rr, :], W[:, first:first + n]).astype(BF16)

    def local_gates():
        rr = chip_rows(y)
        G[rr, :] = mm(XG[rr, :], W[:, o_g:o_g + 128])

    def far_parts(part, chip):
        rr = pl.ds(pl.multiple_of(chip * 2 * R + 2 * third * part, 16), 2 * third)
        return rr, [rows_of(2 * chip + i, part * third, third) for i in range(2)]

    def project_far(part, cols):
        for k in range(1, n_y):
            rr, to = far_parts(part, source(k))
            for first, n in cols:
                res = mm(XG[rr, :], W[:, first:first + n]).astype(BF16)
                for i in range(2):
                    PJ[to[i], first:first + n] = res[i * third:(i + 1) * third]

    def far_gates(part):
        for k in range(1, n_y):
            rr, to = far_parts(part, source(k))
            res = mm(XG[rr, :], W[:, o_g:o_g + 128])
            for i in range(2):
                G[to[i], :] = res[i * third:(i + 1) * third]

    W[:, o_g:o_g + 128] = jnp.concatenate(
        [wig[...].astype(F32), wfg[...].astype(F32), jnp.zeros((128 - 2 * n_heads, D), F32)],
        axis=0).T.astype(BF16)
    for c in kv_copies:
        c.wait()
    own.wait_recv()
    project_local(kv_cols)
    local_gates()
    for c in rest_copies:
        c.wait()
    project_local(rest_cols)
    for part in range(2):
        forward(part)
        forwarded(part)
        project_far(part, kv_cols)
        far_gates(part)
        project_far(part, rest_cols)
    forward(2)
    forward(3)
    forwarded(2)
    forwarded(3)
    for c in small_copies:
        c.wait()
    far_gates(2)

    gt = G[...].T
    in_all, forget_all = gt[0:n_heads], gt[n_heads:2 * n_heads]
    sub = lax.broadcasted_iota(jnp.int32, (n_heads, T), 0)
    sub8 = lax.broadcasted_iota(jnp.int32, (8, T), 0)
    in_pre = jnp.zeros((8, T), F32)
    log_f = jnp.zeros((8, T), F32)
    for h in range(heads):
        head = tp * heads + h
        row_i = jnp.sum(jnp.where(sub == head, in_all, 0.0), axis=0, keepdims=True)
        row_f = jnp.sum(jnp.where(sub == head, forget_all, 0.0), axis=0, keepdims=True) + bias[head]
        row_f = jnp.minimum(row_f, 0.0) - jnp.log1p(jnp.exp(-jnp.abs(row_f))) + extra[h:h + 1, :]
        in_pre = jnp.where(sub8 == h, row_i, in_pre)
        log_f = jnp.where(sub8 == h, row_f, log_f)
    seg = T // 128
    li = lax.broadcasted_iota(jnp.int32, (128, 128), 0)
    lj = lax.broadcasted_iota(jnp.int32, (128, 128), 1)
    tri = jnp.where(li <= lj, 1.0, 0.0).astype(BF16)
    rows = jnp.concatenate([log_f[:, i * 128:(i + 1) * 128] for i in range(seg)], axis=0)
    split, rem = [], rows
    for _ in range(3):
        split.append(rem.astype(BF16))
        rem = rem - split[-1].astype(F32)
    part = mm(jnp.concatenate(split, axis=0), tri)
    n8 = 8 * seg
    part = part[0:n8] + part[n8:2 * n8] + part[2 * n8:3 * n8]
    ends = jnp.broadcast_to(part[:, 127:128], (n8, 128))
    run_cum, base = [], jnp.zeros((8, 128), F32)
    for i in range(seg):
        run_cum.append(part[8 * i:8 * i + 8] + base)
        base = base + ends[8 * i:8 * i + 8]
    cum = jnp.concatenate(run_cum, axis=1)
    gap = in_pre - cum
    decay = cum[:, T - 1:T]
    gmax = jnp.max(gap, axis=1, keepdims=True)
    w_all = jnp.exp(gap - gmax)
    w_hi = w_all.astype(BF16)
    w_lo = (w_all - w_hi.astype(F32)).astype(BF16)
    w_two = jnp.concatenate([w_hi, w_lo], axis=0)
    ones = jnp.ones((1, 128), F32)
    s8 = lax.broadcasted_iota(jnp.int32, (8, 128), 0)
    pr = KEY_DIM // PARTS

    project_far(2, kv_cols)

    def group_copies(k, h, p):
        to = sp - x_in + lax.rem(x_in + k, B)
        if p == 0:
            ref = SM.at[x_in, h]
        else:
            ref = ST.at[x_in, h, pl.ds((p - 1) * pr, pr), :]
        return remote(ref, ref, s_sem, xs_r.at[k - 1, h, p], to_sp=to)

    def group_sends(fn):
        for k in range(1, B):
            pl.when((zg < A - 1) | (x_in + k < B))(functools.partial(fn, k))

    pl.when(sp < n_sp - 1)(lambda: pl.semaphore_wait(ent, n_later))
    for h in range(heads):
        k_t = PJ[:, h * KEY_DIM:(h + 1) * KEY_DIM].T
        keyed = (k_t.astype(F32) * w_all[h:h + 1, :]).astype(BF16)
        n2 = mm(w_two, PJ[:, h * KEY_DIM:(h + 1) * KEY_DIM])
        norm = n2[h:h + 1] + n2[8 + h:9 + h]
        d_row = decay[h:h + 1] * ones
        m_row = (decay[h:h + 1] + gmax[h:h + 1]) * ones
        SM[x_in, h] = jnp.where(s8 == 0, norm, jnp.where(s8 == 1, d_row, m_row))
        ST[x_in, h] = mm(keyed, PJ[:, o_v + h * VALUE_DIM:o_v + (h + 1) * VALUE_DIM]).astype(BF16)

        def go(k, h=h):
            for p in range(PARTS + 1):
                group_copies(k, h, p).start()

        group_sends(go)

    def weights(h, limit):
        valid = [j < limit for j in range(B)]
        ds = [jnp.where(valid[j], SM[j, h, 1:2], 0.0) for j in range(B)]
        ms = [jnp.where(valid[j], SM[j, h, 2:3], NEG) for j in range(B)]
        ns = [jnp.where(valid[j], SM[j, h, 0:1], 0.0) for j in range(B)]
        c_m = jnp.where(zg > 0, CSI[h, 2:3], 0.0)
        c_n = jnp.where(zg > 0, CSI[h, 0:1], first_norm[h:h + 1, :])
        after = [jnp.zeros((1, 128), F32)] * B
        for j in range(B - 2, -1, -1):
            after[j] = after[j + 1] + ds[j + 1]
        c_m = c_m + after[0] + ds[0]
        top = c_m
        for j in range(B):
            top = jnp.maximum(top, ms[j] + after[j])
        c_c = jnp.exp(c_m - top)
        c_j = [jnp.where(valid[j], jnp.exp(ms[j] + after[j] - top), 0.0) for j in range(B)]
        norm = c_c * c_n
        for j in range(B):
            norm = norm + c_j[j] * ns[j]
        return c_c, c_j, valid, norm, top

    def joined(h, c_c, c_j, valid, first, n):
        two = lambda v: jnp.concatenate([v] * (VALUE_DIM // 128), axis=1)
        r = slice(first, first + n)
        mem = two(c_c) * jnp.where(zg > 0, CI[h, r].astype(F32), first_mem[h, r])
        for j in range(B):
            got = ST[j, h, r].astype(F32)
            mem = mem + two(c_j[j]) * (got if valid is None else jnp.where(valid[j], got, 0.0))
        return mem

    def chain_copy(h, p):
        if p == 0:
            s, d = CSO.at[h], CSI.at[h]
        else:
            rr = pl.ds((p - 1) * pr, pr)
            s, d = CO.at[h, rr, :], CI.at[h, rr, :]
        return remote(s, d, s_sem, ch_r.at[h, p], to_sp=sp + B)

    def chain_wait(h, p):
        if p == 0:
            d = CSI.at[h]
        else:
            d = CI.at[h, pl.ds((p - 1) * pr, pr), :]
        remote(d, d, s_sem, ch_r.at[h, p], to_tp=partner).wait_recv()

    def group_wait(k, h, p):
        j = lax.rem(x_in + B - k, B)
        d = SM.at[j, h] if p == 0 else ST.at[j, h, pl.ds((p - 1) * pr, pr), :]
        remote(d, d, s_sem, xs_r.at[k - 1, h, p], to_tp=partner).wait_recv()

    def relay(chained, messages):
        for h, p in messages:
            for k in range(1, B):
                group_wait(k, h, p)
            if chained:
                chain_wait(h, p)
            if p == 0:
                c_c, c_j, _, norm, top = weights(h, B)
                CW[h, 0:1] = c_c
                for j in range(B):
                    CW[h, j + 1:j + 2] = c_j[j]
                CSO[h] = jnp.where(s8 == 0, norm, top)
            else:
                c_j = [CW[h, j + 1:j + 2] for j in range(B)]
                mem = joined(h, CW[h, 0:1], c_j, None, (p - 1) * pr, pr)
                CO[h, (p - 1) * pr:p * pr] = mem.astype(BF16)
            chain_copy(h, p).start()

    messages = [(h, p) for h in range(heads) for p in range(PARTS + 1)]
    last = min(MAX_SLOTS, A - 1)
    left = [list(messages) for _ in range(last)]

    def pass_on(z, n):
        if z < last and left[z]:
            now, left[z] = left[z][:n], left[z][n:]
            pl.when(zg == z)(functools.partial(relay, z > 0, now))

    def pass_rest():
        for z in range(last):
            pass_on(z, len(messages))
        if A - 1 > last:
            pl.when((zg >= last) & (zg < A - 1))(functools.partial(relay, True, messages))

    def end_wait(h):
        @pl.when(zg == A - 1)
        def _():
            for p in range(PARTS + 1):
                for k in range(1, B):
                    pl.when(k <= x_in)(functools.partial(group_wait, k, h, p))
                if A > 1:
                    chain_wait(h, p)

    rb = 256 if T % 256 == 0 else R
    q_scale = KEY_DIM ** -0.5
    shifted = gap + math.log(q_scale)

    def work_running_max():
        run = jnp.concatenate([gap[:, i * 128:(i + 1) * 128] for i in range(seg)], axis=0)
        lane8 = lax.broadcasted_iota(jnp.int32, (n8, 128), 1)
        for d in scan_steps(128):
            run = jnp.maximum(run, jnp.where(lane8 >= d, pltpu.roll(run, d, 1), run))
        ends = jnp.broadcast_to(run[:, 127:128], (n8, 128))
        runs = [run[0:8]]
        ends_top = ends[0:8]
        for i in range(1, seg):
            runs.append(jnp.maximum(run[8 * i:8 * i + 8], ends_top))
            ends_top = jnp.maximum(ends_top, ends[8 * i:8 * i + 8])
        run = jnp.concatenate(runs, axis=1)
        for h in range(heads):
            RM[h] = jnp.broadcast_to(run[h:h + 1], (128, T)).T

    def halo_copy(to):
        return remote(halo_out, halo_in, s_sem, hl_r, to_sp=to)

    def work_product():
        for r0 in range(0, T, rb):
            left = PJ[r0:r0 + rb, o_c + channels:o_c + 2 * channels].astype(F32)
            right = PJ[r0:r0 + rb, o_c + 2 * channels:o_c + 3 * channels].astype(F32)
            prod = (left * right).astype(BF16)
            PROD[8 + r0:8 + r0 + rb, :] = prod.astype(F32)
            if r0 + rb == T:
                halo_out[...] = prod[rb - 16:rb]
        pl.when(sp < n_sp - 1)(lambda: halo_copy(sp + 1).start())

    def attend(h, r0):
        e = r0 + rb
        q = PJ[r0:e, o_q + h * KEY_DIM:o_q + (h + 1) * KEY_DIM]
        k = PJ[0:e, h * KEY_DIM:(h + 1) * KEY_DIM]
        v = PJ[0:e, o_v + h * VALUE_DIM:o_v + (h + 1) * VALUE_DIM]
        s = mm_t(q, k)
        ti = lax.broadcasted_iota(jnp.int32, (rb, rb), 0)
        si = lax.broadcasted_iota(jnp.int32, (rb, rb), 1)
        rm = RM[h, r0:e, :]
        w = shifted[h:h + 1, 0:e] - jnp.concatenate([rm] * (e // 128), axis=1)
        diag = jnp.where(ti >= si, w[:, r0:e], NEG)
        w = jnp.concatenate([w[:, 0:r0], diag], axis=1) if r0 else diag
        mix = s * jnp.exp(w)
        DEN[h, r0:e, :] = jnp.broadcast_to(jnp.sum(mix, axis=1, keepdims=True), (rb, 128))
        NUM[r0:e, h * VALUE_DIM:(h + 1) * VALUE_DIM] = mm(mix.astype(BF16), v)

    def conv_finish():
        @pl.when(sp > 0)
        def _():
            halo_copy(sp).wait_recv()
            PROD[0:8, :] = halo_in[...].astype(F32)[8:16]

        @pl.when(sp == 0)
        def _():
            PROD[0:8, :] = jnp.zeros((8, channels), F32)

        tap = taps[:, pl.ds(pl.multiple_of(tp * channels, 128), channels)]
        for r0 in range(0, T, rb):
            f = tap[0:1] * PROD[6 + r0:6 + r0 + rb, :]
            f = f + tap[1:2] * PROD[7 + r0:7 + r0 + rb, :]
            f = f + tap[2:3] * PROD[8 + r0:8 + r0 + rb, :]
            gate = PJ[r0:r0 + rb, o_c:o_c + channels].astype(F32)
            CB[r0:r0 + rb, :] = (gate * f).astype(BF16)

    cw = D // RS_CHUNKS
    chips = [y] + [lax.rem(y + k, n_y) for k in range(1, n_y)]
    order = list(range(1, n_y)) + [0]

    def conv_copy(idx):
        return remote(PSC.at[rows_of(2 * chips[idx] + 1 - core), :], DRC.at[idx], s_sem, cd_r.at[idx],
                      to_tp=partner)

    def conv_out(idx, q):
        rr = chip_rows(chips[idx])
        for j in range(q * RS_CHUNKS // 2, (q + 1) * RS_CHUNKS // 2):
            cols = slice(j * cw, (j + 1) * cw)
            PSC[rr, cols] = mm(CB[rr, :], WO[vw:, cols]).astype(BF16)
        if q == 1:
            conv_copy(idx).start()

    early = EARLY * cw

    def early_copy(k):
        return remote(YC.at[k - 1], YCR.at[k - 1], s_sem, yc_r.at[k - 1],
                      to_tp=lax.rem(y + k, n_y) * 2 + core)

    def conv_early():
        for k in range(1, n_y):
            conv_copy(k).wait_recv()
            mine = rows_of(2 * chips[k] + core)
            s = PSC[mine, 0:early].astype(F32) + DRC[k, :, 0:early].astype(F32)
            YC[k - 1] = s.astype(BF16)
            early_copy(k).start()

    work_running_max()
    project_far(2, rest_cols)
    work_product()
    for h in range(heads):
        for r0 in range(0, T, rb):
            attend(h, r0)
    pass_on(0, 10)
    pass_on(1, 10)
    conv_finish()
    for c in out_copies:
        c.wait()
    for idx in order[:-1]:
        for q in range(2):
            conv_out(idx, q)
    pass_on(2, 10)
    for idx in order[-1:]:
        for q in range(2):
            conv_out(idx, q)
    conv_early()
    pass_rest()

    parts = [(0, EARLY), (EARLY, RS_CHUNKS // 2), (RS_CHUNKS // 2, RS_CHUNKS)]
    per_chip = -(-2 * R // 128)

    def mem_copy(idx, q):
        cols = pl.ds(parts[q][0] * cw, (parts[q][1] - parts[q][0]) * cw)
        return remote(PSM.at[rows_of(2 * chips[idx] + 1 - core), cols], DRM.at[idx, :, cols],
                      s_sem, rd_r.at[idx, q], to_tp=partner)

    def mem_out(idx, q):
        rr = chip_rows(chips[idx])
        for j in range(*parts[q]):
            cols = slice(j * cw, (j + 1) * cw)
            PSM[rr, cols] = mm(MO[rr, :], WO[0:vw, cols]).astype(BF16)
        mem_copy(idx, q).start()

    sq_out[...] = jnp.zeros_like(sq_out)
    sq = [None] * n_y
    for h in range(heads):
        end_wait(h)
        wts = weights(h, x_in)
        c_mem = joined(h, *wts[:3], 0, KEY_DIM)
        c_norm, cmax = wts[3], wts[4]
        hi = c_mem.astype(BF16)
        lo = (c_mem - hi.astype(F32)).astype(BF16)
        two = jnp.concatenate([hi, lo], axis=0)
        n_col = jnp.broadcast_to(c_norm, (128, 128)).T
        n_hi = n_col.astype(BF16)
        n_lo = (n_col - n_hi.astype(F32)).astype(BF16)
        n_two = jnp.concatenate([n_hi, n_lo], axis=0)
        for idx in order:
            rr = chip_rows(chips[idx])
            q = PJ[rr, o_q + h * KEY_DIM:o_q + (h + 1) * KEY_DIM]
            qq = jnp.concatenate([q, q], axis=1)
            fm = mm(qq, two)
            fn = mm(qq, n_two)
            m0 = RM[h, rr, :]
            m = jnp.maximum(m0, cmax)
            k0 = jnp.exp(m0 - m)
            k1 = jnp.exp(cmax - m) * q_scale
            den = k0 * DEN[h, rr, :] + k1 * fn
            inv = 1.0 / jnp.maximum(jnp.abs(den), 1.0)
            k0, k1 = k0 * inv, k1 * inv
            cols = slice(h * VALUE_DIM, (h + 1) * VALUE_DIM)
            mo = (jnp.concatenate([k0, k0], axis=1) * NUM[rr, cols]
                  + jnp.concatenate([k1, k1], axis=1) * fm)
            MO[rr, cols] = mo.astype(BF16)
            s2 = mo * mo
            s2 = s2[:, 0:128] + s2[:, 128:256]
            sq[idx] = s2 if sq[idx] is None else sq[idx] + s2
            if h == heads - 1 and idx > 0:
                mem_out(idx, 0)
    for idx in range(n_y):
        for i in range(per_chip):
            n = min(128, 2 * R - i * 128)
            row = jnp.sum(sq[idx][i * 128:i * 128 + n].T, axis=0, keepdims=True)
            sq_out[pl.ds(chips[idx] * per_chip + i, 1), 0:n] = row
    for k in range(1, n_tp):
        cp = remote(sq_out, sq_in.at[k - 1], s_sem, sq_r, to_tp=lax.rem(tp + k, n_tp))
        cp.start()
        sends.append(cp)

    def cols_of(j):
        return pl.ds(j * cw, cw)

    def y_copy(k, j):
        return remote(YS.at[k - 1, :, cols_of(j)], YR.at[k - 1, :, cols_of(j)], s_sem,
                      ry_r.at[k - 1, j], to_tp=lax.rem(y + k, n_y) * 2 + core)

    def mem_sum(idx, j):
        cols = slice(j * cw, (j + 1) * cw)
        mine = rows_of(2 * chips[idx] + core)
        return PSM[mine, cols].astype(F32) + DRM[idx, :, cols].astype(F32)

    for idx in order[:-1]:
        mem_out(idx, 1)
    for k in range(1, n_y):
        mem_copy(k, 0).wait_recv()
        for j in range(EARLY):
            YS[k - 1, :, j * cw:(j + 1) * cw] = mem_sum(k, j).astype(BF16)
            y_copy(k, j).start()
    for idx in order[:-1]:
        mem_out(idx, 2)
    for q in range(3):
        mem_out(0, q)

    tot = sq_out[...]
    remote(sq_in, sq_in, s_sem, sq_r, to_tp=partner).wait_recv()
    for k in range(1, n_tp):
        tot = tot + sq_in[k - 1]
    r_scale = lax.rsqrt(tot / float(width) + EPS)
    for c in range(n_y):
        for i in range(per_chip):
            n = min(128, 2 * R - i * 128)
            at = c * 2 * R + i * 128
            RC[at:at + n, :] = jnp.broadcast_to(r_scale[c * per_chip + i:c * per_chip + i + 1, 0:n], (128, n)).T

    def row_scale(idx):
        return jnp.concatenate([RC[rows_of(2 * chips[idx] + core), :]] * (cw // 128), axis=1)

    def chip_sum(idx, j):
        cols = slice(j * cw, (j + 1) * cw)
        mine = rows_of(2 * chips[idx] + core)
        s = PSC[mine, cols].astype(F32) + DRC[idx, :, cols].astype(F32)
        return s + mem_sum(idx, j) * row_scale(idx)

    for k in range(1, n_y):
        for q in range(1, 3):
            mem_copy(k, q).wait_recv()
        for j in range(EARLY, RS_CHUNKS):
            YS[k - 1, :, j * cw:(j + 1) * cw] = chip_sum(k, j).astype(BF16)
            y_copy(k, j).start()
    conv_copy(0).wait_recv()
    for q in range(3):
        mem_copy(0, q).wait_recv()
    for k in range(1, n_y):
        early_copy(k).wait_recv()
    for j in range(RS_CHUNKS):
        s = chip_sum(0, j)
        for k in range(1, n_y):
            y_copy(k, j).wait_recv()
            got = YR[k - 1, :, j * cw:(j + 1) * cw].astype(F32)
            if j < EARLY:
                got = got * row_scale(0) + YCR[k - 1, :, j * cw:(j + 1) * cw].astype(F32)
            s = s + got
        out[:, j * cw:(j + 1) * cw] = s.astype(BF16)

    for cp in sends:
        cp.wait_send()
    own.wait_send()
    for h in range(heads):
        for p in range(PARTS + 1):
            group_sends(lambda k, h=h, p=p: group_copies(k, h, p).wait_send())

            @pl.when(zg < A - 1)
            def _(h=h, p=p):
                chain_copy(h, p).wait_send()
    pl.when(sp < n_sp - 1)(lambda: halo_copy(sp + 1).wait_send())
    for idx in range(n_y):
        conv_copy(idx).wait_send()
        for q in range(3):
            mem_copy(idx, q).wait_send()
    for k in range(1, n_y):
        early_copy(k).wait_send()
        for j in range(RS_CHUNKS):
            y_copy(k, j).wait_send()


def per_device(
    n_sp, n_tp,
    tokens, in_gain, w_query, w_key, w_value, w_input_gate, w_forget_gate, forget_bias,
    forget_extra, w_conv_gate, w_conv_left, w_conv_right, conv_taps, first_memory, first_norm,
    w_out_memory, w_out_conv,
):
    heads = w_query.shape[1] // KEY_DIM
    channels = w_conv_gate.shape[1]
    R, D = tokens.shape
    T = R * n_tp
    n_y = n_tp // 2
    qk, vw = heads * KEY_DIM, heads * VALUE_DIM
    total = 2 * qk + vw + 128 + 3 * channels
    n_heads = w_input_gate.shape[1]
    B = group_size(n_sp)
    hbm = pl.BlockSpec(memory_space=pl.ANY)
    V, dma = pltpu.VMEM, pltpu.SemaphoreType.DMA
    ny1 = n_y - 1
    np_ = len(gather_pieces(R))
    sq_rows = -(-(n_y * -(-2 * R // 128)) // 8) * 8
    early = EARLY * D // RS_CHUNKS
    return pl.pallas_call(
        functools.partial(kernel, n_sp, n_tp, heads, channels, n_heads * VALUE_DIM),
        out_shape=pltpu.VMEM((R, D), BF16),
        in_specs=[hbm] * 17,
        out_specs=pl.BlockSpec(memory_space=pltpu.VMEM),
        scratch_shapes=[
            V((R, D), BF16), V((1, D), F32), V((n_heads, D), BF16), V((n_heads, D), BF16),
            pltpu.SMEM((n_heads,), F32), V((heads, T), F32), V((TAPS, n_tp * channels), F32),
            V((heads, KEY_DIM, VALUE_DIM), F32), V((heads, KEY_DIM), F32),
            V((D, total), BF16), V((vw + channels, D), BF16), V((T, D), BF16), V((T, total), BF16),
            V((T, 128), F32), V((heads, T, 128), F32), V((T, vw), F32), V((heads, T, 128), F32),
            V((T, vw), BF16), V((T, channels), BF16), V((8 + T, channels), F32),
            V((16, channels), BF16), V((16, channels), BF16),
            V((B, heads, KEY_DIM, VALUE_DIM), BF16), V((B, heads, 8, 128), F32),
            V((heads, KEY_DIM, VALUE_DIM), BF16), V((heads, KEY_DIM, VALUE_DIM), BF16),
            V((heads, 8, 128), F32), V((heads, 8, 128), F32), V((heads, 8 * -(-(B + 1) // 8), 128), F32),
            V((sq_rows, 128), F32), V((n_tp - 1, sq_rows, 128), F32), V((T, 128), F32),
            V((T, D), BF16), V((T, D), BF16), V((n_y, R, D), BF16), V((n_y, R, D), BF16),
            V((ny1, R, D), BF16), V((ny1, R, D), BF16),
            V((ny1, R, early), BF16), V((ny1, R, early), BF16),
            dma((7,)), dma, dma, dma((ny1, np_)), dma((ny1, np_)), dma((B - 1, heads, PARTS + 1)),
            dma((heads, PARTS + 1)), dma, dma, dma((n_y,)), dma((n_y, 3)), dma((ny1, RS_CHUNKS)), dma((ny1,)),
            pltpu.SemaphoreType.REGULAR,
        ],
        compiler_params=pltpu.CompilerParams(
            collective_id=0, has_side_effects=True, vmem_limit_bytes=60 * 1024 * 1024),
        name="layer",
    )(
        tokens, in_gain.reshape(1, D), w_key, w_value, w_query, w_conv_gate, w_conv_left,
        w_conv_right, w_input_gate.T, w_forget_gate.T, forget_bias, forget_extra.T, conv_taps, first_memory, first_norm,
        w_out_memory, w_out_conv,
    )


def solution(mesh):
    in_specs = (
        P(("sp", "tp"), None), P(), P(None, "tp"), P(None, "tp"), P(None, "tp"), P(), P(), P(),
        P("sp", "tp"), P(None, "tp"), P(None, "tp"), P(None, "tp"), P(), P("tp", None, None),
        P("tp", None), P("tp", None), P("tp", None),
    )
    return jax.shard_map(
        functools.partial(per_device, mesh.shape["sp"], mesh.shape["tp"]),
        mesh=mesh, in_specs=in_specs, out_specs=P(("sp", "tp"), None), check_vma=False,
    )
```

```python
import functools
import math

import jax
import jax.numpy as jnp
from jax import lax
from jax.experimental import pallas as pl
from jax.experimental.pallas import tpu as pltpu
from jax.sharding import PartitionSpec as P

KEY_DIM = 128
VALUE_DIM = 256
TAPS = 3
EPS = 1e-06
NEG = -1e30
MESH = pl.DeviceIdType.MESH
F32 = jnp.float32
BF16 = jnp.bfloat16
RS_CHUNKS = 8
EARLY = 1
PARTS = 4
MAX_SLOTS = 3


def mm(a, b):
    return lax.dot_general(a, b, (((1,), (0,)), ((), ())), preferred_element_type=F32)


def mm_t(a, b):
    return lax.dot_general(a, b, (((1,), (1,)), ((), ())), preferred_element_type=F32)


def scan_steps(n):
    steps, d = [], 1
    while d < n:
        steps.append(d)
        d *= 2
    return steps


def group_size(n_sp):
    b = 1
    while (2 * b) ** 2 <= n_sp and n_sp % (2 * b) == 0:
        b *= 2
    return b


def gather_pieces(rows):
    third = rows // 3
    return [(0, third), (third, third), (2 * third, third - 16), (rows - 16, 16)]


def kernel(
    n_sp, n_tp, heads, channels, width,
    tokens_h, gain_h, wk, wv, wq, wcg, wcl, wcr, wig_h, wfg_h, bias_h, extra_h, taps_h, first_mem_h, first_norm_h,
    wom, woc, out,
    TK, gain, wig, wfg, bias, extra, taps, first_mem, first_norm,
    W, WO, XG, PJ, G, RM, NUM, DEN, MO, CB, PROD, halo_out, halo_in,
    ST, SM, CO, CI, CSO, CSI, CW, sq_out, sq_in, RC,
    PSC, PSM, DRC, DRM, YS, YR, YC, YCR,
    i_sem, s_sem, ag_d, ag_yr, ag_fr, xs_r, ch_r, hl_r, sq_r, cd_r, rd_r, ry_r, yc_r, ent,
):
    sp = lax.axis_index("sp")
    tp = lax.axis_index("tp")
    core = lax.rem(tp, 2)
    y = tp // 2
    n_y = n_tp // 2
    partner = tp + 1 - 2 * core
    R, D = TK.shape
    T = R * n_tp
    B = group_size(n_sp)
    A = n_sp // B
    zg, x_in = sp // B, lax.rem(sp, B)
    qk, vw = heads * KEY_DIM, heads * VALUE_DIM
    o_v, o_g = qk, qk + vw
    o_q = o_g + 128
    o_c = o_q + qk
    total = o_c + 3 * channels
    n_heads = wig.shape[0]

    def remote(src, dst, ss, rs, to_tp=None, to_sp=None):
        return pltpu.make_async_remote_copy(
            src_ref=src, dst_ref=dst, send_sem=ss, recv_sem=rs,
            device_id=(sp if to_sp is None else to_sp, tp if to_tp is None else to_tp),
            device_id_type=MESH,
        )

    barrier = pltpu.get_barrier_semaphore()
    for k in range(1, n_tp):
        pl.semaphore_signal(barrier, inc=1, device_id=(sp, lax.rem(tp + k, n_tp)), device_id_type=MESH)

    def later(fn):
        for k in range(1, B):
            pl.when(x_in + k < B)(functools.partial(fn, k))
        pl.when(zg < A - 1)(functools.partial(fn, B))
        if B > 1:
            pl.when((x_in == B - 1) & (zg < A - 1))(functools.partial(fn, 1))

    def earlier(fn):
        for k in range(1, B):
            pl.when(x_in >= k)(functools.partial(fn, k))
        pl.when(zg > 0)(functools.partial(fn, B))
        if B > 1:
            pl.when((x_in == 0) & (zg > 0))(functools.partial(fn, 1))

    extra_link = 1 if B > 1 else 0
    n_earlier = x_in + jnp.where(zg > 0, 1, 0) + extra_link * jnp.where((x_in == 0) & (zg > 0), 1, 0)
    n_later = (B - 1 - x_in + jnp.where(zg < A - 1, 1, 0)
               + extra_link * jnp.where((x_in == B - 1) & (zg < A - 1), 1, 0))
    later(lambda k: pl.semaphore_signal(barrier, inc=1, device_id=(sp + k, tp), device_id_type=MESH))

    third = R // 3

    def copies(sem, pairs):
        return [pltpu.make_async_copy(a, b, i_sem.at[sem]) for a, b in pairs]

    token_copies = [copies(i, [(tokens_h.at[r, :], TK.at[r, :])])[0]
                    for i, r in enumerate([pl.ds(0, third), pl.ds(third, R - third)])]
    gate_copies = copies(2, [(gain_h, gain), (wig_h, wig), (wfg_h, wfg)])
    kv_copies = copies(3, [(wk, W.at[:, pl.ds(0, qk)]), (wv, W.at[:, pl.ds(o_v, vw)])])
    small_copies = copies(4, [(bias_h, bias), (extra_h, extra), (taps_h, taps),
                              (first_mem_h, first_mem), (first_norm_h, first_norm)])
    rest_copies = copies(5, [(wq, W.at[:, pl.ds(o_q, qk)])] + [
        (w, W.at[:, pl.ds(o_c + i * channels, channels)]) for i, w in enumerate((wcg, wcl, wcr))])
    out_copies = copies(6, [(woc, WO.at[pl.ds(vw, channels), :]), (wom, WO.at[pl.ds(0, vw), :])])
    for c in token_copies[:1] + gate_copies + token_copies[1:]:
        c.start()

    def rows_of(block, first=0, n=None):
        n = R if n is None else n
        return pl.ds(pl.multiple_of(block * R + first, 16), n)

    def chip_rows(chip):
        return pl.ds(pl.multiple_of(chip * 2 * R, 16), 2 * R)

    pieces = gather_pieces(R)
    sends = []

    def far_rows(chip, c, src_core):
        first, n = pieces[c]
        part = min(c, 2)
        at = chip * 2 * R + 2 * third * part + src_core * third + (first - part * third)
        return pl.ds(pl.multiple_of(at, 16), n)

    def y_piece(k, c, chip, to):
        src = XG.at[rows_of(tp, pieces[c][0], pieces[c][1]), :]
        return remote(src, XG.at[far_rows(chip, c, core), :], s_sem, ag_yr.at[k - 1, c], to_tp=to)

    for c in gate_copies:
        c.wait()
    for c, (first, n) in enumerate(pieces):
        if c < 2:
            token_copies[c].wait()
        x = TK[first:first + n, :].astype(F32)
        scale = lax.rsqrt(jnp.mean(x * x, axis=1, keepdims=True) + EPS)
        XG[rows_of(tp, first, n), :] = (x * scale * gain[...]).astype(BF16)
        if c == 0:
            pl.semaphore_wait(barrier, n_tp - 1 + n_earlier)
        if c == 0 or c == len(pieces) - 1:
            for cc in [0] if c == 0 else range(1, len(pieces)):
                for k in range(1, n_y):
                    cp = y_piece(k, cc, y, lax.rem(y + k, n_y) * 2 + core)
                    cp.start()
                    sends.append(cp)
    for c in kv_copies + small_copies + rest_copies + out_copies:
        c.start()
    earlier(lambda k: pl.semaphore_signal(ent, inc=1, device_id=(sp - k, tp), device_id_type=MESH))
    own = remote(XG.at[rows_of(tp), :], XG.at[rows_of(tp), :], s_sem, ag_d, to_tp=partner)
    own.start()

    def source(k):
        return lax.rem(y + n_y - k, n_y)

    def forward(c):
        for k in range(1, n_y):
            chip = source(k)
            y_piece(k, c, chip, partner).wait_recv()
            r = far_rows(chip, c, core)
            cp = remote(XG.at[r, :], XG.at[r, :], s_sem, ag_fr.at[k - 1, c], to_tp=partner)
            cp.start()
            sends.append(cp)

    def forwarded(c):
        for k in range(1, n_y):
            r = far_rows(source(k), c, 1 - core)
            remote(XG.at[r, :], XG.at[r, :], s_sem, ag_fr.at[k - 1, c], to_tp=partner).wait_recv()

    kv_cols = [(0, o_g)]
    rest_cols = [(o_q, qk)] + [(o_c + i * channels, channels) for i in range(3)]

    def project_local(cols):
        rr = chip_rows(y)
        for first, n in cols:
            PJ[rr, first:first + n] = mm(XG[rr, :], W[:, first:first + n]).astype(BF16)

    def local_gates():
        rr = chip_rows(y)
        G[rr, :] = mm(XG[rr, :], W[:, o_g:o_g + 128])

    def far_parts(part, chip):
        rr = pl.ds(pl.multiple_of(chip * 2 * R + 2 * third * part, 16), 2 * third)
        return rr, [rows_of(2 * chip + i, part * third, third) for i in range(2)]

    def project_far(part, cols):
        for k in range(1, n_y):
            rr, to = far_parts(part, source(k))
            for first, n in cols:
                res = mm(XG[rr, :], W[:, first:first + n]).astype(BF16)
                for i in range(2):
                    PJ[to[i], first:first + n] = res[i * third:(i + 1) * third]

    def far_gates(part):
        for k in range(1, n_y):
            rr, to = far_parts(part, source(k))
            res = mm(XG[rr, :], W[:, o_g:o_g + 128])
            for i in range(2):
                G[to[i], :] = res[i * third:(i + 1) * third]

    W[:, o_g:o_g + 128] = jnp.concatenate(
        [wig[...].astype(F32), wfg[...].astype(F32), jnp.zeros((128 - 2 * n_heads, D), F32)],
        axis=0).T.astype(BF16)
    for c in kv_copies:
        c.wait()
    own.wait_recv()
    project_local(kv_cols)
    local_gates()
    for c in rest_copies:
        c.wait()
    project_local(rest_cols)
    for part in range(2):
        forward(part)
        forwarded(part)
        project_far(part, kv_cols)
        far_gates(part)
        project_far(part, rest_cols)
    forward(2)
    forward(3)
    forwarded(2)
    forwarded(3)
    for c in small_copies:
        c.wait()
    far_gates(2)

    gt = G[...].T
    in_all, forget_all = gt[0:n_heads], gt[n_heads:2 * n_heads]
    sub = lax.broadcasted_iota(jnp.int32, (n_heads, T), 0)
    sub8 = lax.broadcasted_iota(jnp.int32, (8, T), 0)
    in_pre = jnp.zeros((8, T), F32)
    log_f = jnp.zeros((8, T), F32)
    for h in range(heads):
        head = tp * heads + h
        row_i = jnp.sum(jnp.where(sub == head, in_all, 0.0), axis=0, keepdims=True)
        row_f = jnp.sum(jnp.where(sub == head, forget_all, 0.0), axis=0, keepdims=True) + bias[head]
        row_f = jnp.minimum(row_f, 0.0) - jnp.log1p(jnp.exp(-jnp.abs(row_f))) + extra[h:h + 1, :]
        in_pre = jnp.where(sub8 == h, row_i, in_pre)
        log_f = jnp.where(sub8 == h, row_f, log_f)
    seg = T // 128
    li = lax.broadcasted_iota(jnp.int32, (128, 128), 0)
    lj = lax.broadcasted_iota(jnp.int32, (128, 128), 1)
    tri = jnp.where(li <= lj, 1.0, 0.0).astype(BF16)
    rows = jnp.concatenate([log_f[:, i * 128:(i + 1) * 128] for i in range(seg)], axis=0)
    split, rem = [], rows
    for _ in range(3):
        split.append(rem.astype(BF16))
        rem = rem - split[-1].astype(F32)
    part = mm(jnp.concatenate(split, axis=0), tri)
    n8 = 8 * seg
    part = part[0:n8] + part[n8:2 * n8] + part[2 * n8:3 * n8]
    ends = jnp.broadcast_to(part[:, 127:128], (n8, 128))
    run_cum, base = [], jnp.zeros((8, 128), F32)
    for i in range(seg):
        run_cum.append(part[8 * i:8 * i + 8] + base)
        base = base + ends[8 * i:8 * i + 8]
    cum = jnp.concatenate(run_cum, axis=1)
    gap = in_pre - cum
    decay = cum[:, T - 1:T]
    gmax = jnp.max(gap, axis=1, keepdims=True)
    w_all = jnp.exp(gap - gmax)
    w_hi = w_all.astype(BF16)
    w_lo = (w_all - w_hi.astype(F32)).astype(BF16)
    w_two = jnp.concatenate([w_hi, w_lo], axis=0)
    ones = jnp.ones((1, 128), F32)
    s8 = lax.broadcasted_iota(jnp.int32, (8, 128), 0)
    pr = KEY_DIM // PARTS

    project_far(2, kv_cols)

    def group_copies(k, h, p):
        to = sp - x_in + lax.rem(x_in + k, B)
        if p == 0:
            ref = SM.at[x_in, h]
        else:
            ref = ST.at[x_in, h, pl.ds((p - 1) * pr, pr), :]
        return remote(ref, ref, s_sem, xs_r.at[k - 1, h, p], to_sp=to)

    def group_sends(fn):
        for k in range(1, B):
            pl.when((zg < A - 1) | (x_in + k < B))(functools.partial(fn, k))

    pl.when(sp < n_sp - 1)(lambda: pl.semaphore_wait(ent, n_later))
    for h in range(heads):
        k_t = PJ[:, h * KEY_DIM:(h + 1) * KEY_DIM].T
        keyed = (k_t.astype(F32) * w_all[h:h + 1, :]).astype(BF16)
        n2 = mm(w_two, PJ[:, h * KEY_DIM:(h + 1) * KEY_DIM])
        norm = n2[h:h + 1] + n2[8 + h:9 + h]
        d_row = decay[h:h + 1] * ones
        m_row = (decay[h:h + 1] + gmax[h:h + 1]) * ones
        SM[x_in, h] = jnp.where(s8 == 0, norm, jnp.where(s8 == 1, d_row, m_row))
        ST[x_in, h] = mm(keyed, PJ[:, o_v + h * VALUE_DIM:o_v + (h + 1) * VALUE_DIM]).astype(BF16)

        def go(k, h=h):
            for p in range(PARTS + 1):
                group_copies(k, h, p).start()

        group_sends(go)

    def weights(h, limit):
        valid = [j < limit for j in range(B)]
        ds = [jnp.where(valid[j], SM[j, h, 1:2], 0.0) for j in range(B)]
        ms = [jnp.where(valid[j], SM[j, h, 2:3], NEG) for j in range(B)]
        ns = [jnp.where(valid[j], SM[j, h, 0:1], 0.0) for j in range(B)]
        c_m = jnp.where(zg > 0, CSI[h, 2:3], 0.0)
        c_n = jnp.where(zg > 0, CSI[h, 0:1], first_norm[h:h + 1, :])
        after = [jnp.zeros((1, 128), F32)] * B
        for j in range(B - 2, -1, -1):
            after[j] = after[j + 1] + ds[j + 1]
        c_m = c_m + after[0] + ds[0]
        top = c_m
        for j in range(B):
            top = jnp.maximum(top, ms[j] + after[j])
        c_c = jnp.exp(c_m - top)
        c_j = [jnp.where(valid[j], jnp.exp(ms[j] + after[j] - top), 0.0) for j in range(B)]
        norm = c_c * c_n
        for j in range(B):
            norm = norm + c_j[j] * ns[j]
        return c_c, c_j, valid, norm, top

    def joined(h, c_c, c_j, valid, first, n):
        two = lambda v: jnp.concatenate([v] * (VALUE_DIM // 128), axis=1)
        r = slice(first, first + n)
        mem = two(c_c) * jnp.where(zg > 0, CI[h, r].astype(F32), first_mem[h, r])
        for j in range(B):
            got = ST[j, h, r].astype(F32)
            mem = mem + two(c_j[j]) * (got if valid is None else jnp.where(valid[j], got, 0.0))
        return mem

    def chain_copy(h, p):
        if p == 0:
            s, d = CSO.at[h], CSI.at[h]
        else:
            rr = pl.ds((p - 1) * pr, pr)
            s, d = CO.at[h, rr, :], CI.at[h, rr, :]
        return remote(s, d, s_sem, ch_r.at[h, p], to_sp=sp + B)

    def chain_wait(h, p):
        if p == 0:
            d = CSI.at[h]
        else:
            d = CI.at[h, pl.ds((p - 1) * pr, pr), :]
        remote(d, d, s_sem, ch_r.at[h, p], to_tp=partner).wait_recv()

    def group_wait(k, h, p):
        j = lax.rem(x_in + B - k, B)
        d = SM.at[j, h] if p == 0 else ST.at[j, h, pl.ds((p - 1) * pr, pr), :]
        remote(d, d, s_sem, xs_r.at[k - 1, h, p], to_tp=partner).wait_recv()

    def relay(chained, messages):
        for h, p in messages:
            for k in range(1, B):
                group_wait(k, h, p)
            if chained:
                chain_wait(h, p)
            if p == 0:
                c_c, c_j, _, norm, top = weights(h, B)
                CW[h, 0:1] = c_c
                for j in range(B):
                    CW[h, j + 1:j + 2] = c_j[j]
                CSO[h] = jnp.where(s8 == 0, norm, top)
            else:
                c_j = [CW[h, j + 1:j + 2] for j in range(B)]
                mem = joined(h, CW[h, 0:1], c_j, None, (p - 1) * pr, pr)
                CO[h, (p - 1) * pr:p * pr] = mem.astype(BF16)
            chain_copy(h, p).start()

    messages = [(h, p) for h in range(heads) for p in range(PARTS + 1)]
    last = min(MAX_SLOTS, A - 1)
    left = [list(messages) for _ in range(last)]

    def pass_on(z, n):
        if z < last and left[z]:
            now, left[z] = left[z][:n], left[z][n:]
            pl.when(zg == z)(functools.partial(relay, z > 0, now))

    def pass_rest():
        for z in range(last):
            pass_on(z, len(messages))
        if A - 1 > last:
            pl.when((zg >= last) & (zg < A - 1))(functools.partial(relay, True, messages))

    def end_wait(h):
        @pl.when(zg == A - 1)
        def _():
            for p in range(PARTS + 1):
                for k in range(1, B):
                    pl.when(k <= x_in)(functools.partial(group_wait, k, h, p))
                if A > 1:
                    chain_wait(h, p)

    rb = 256 if T % 256 == 0 else R
    q_scale = KEY_DIM ** -0.5
    shifted = gap + math.log(q_scale)

    def work_running_max():
        run = jnp.concatenate([gap[:, i * 128:(i + 1) * 128] for i in range(seg)], axis=0)
        lane8 = lax.broadcasted_iota(jnp.int32, (n8, 128), 1)
        for d in scan_steps(128):
            run = jnp.maximum(run, jnp.where(lane8 >= d, pltpu.roll(run, d, 1), run))
        ends = jnp.broadcast_to(run[:, 127:128], (n8, 128))
        runs = [run[0:8]]
        ends_top = ends[0:8]
        for i in range(1, seg):
            runs.append(jnp.maximum(run[8 * i:8 * i + 8], ends_top))
            ends_top = jnp.maximum(ends_top, ends[8 * i:8 * i + 8])
        run = jnp.concatenate(runs, axis=1)
        for h in range(heads):
            RM[h] = jnp.broadcast_to(run[h:h + 1], (128, T)).T

    def halo_copy(to):
        return remote(halo_out, halo_in, s_sem, hl_r, to_sp=to)

    def work_product():
        for r0 in range(0, T, rb):
            left = PJ[r0:r0 + rb, o_c + channels:o_c + 2 * channels].astype(F32)
            right = PJ[r0:r0 + rb, o_c + 2 * channels:o_c + 3 * channels].astype(F32)
            prod = (left * right).astype(BF16)
            PROD[8 + r0:8 + r0 + rb, :] = prod.astype(F32)
            if r0 + rb == T:
                halo_out[...] = prod[rb - 16:rb]
        pl.when(sp < n_sp - 1)(lambda: halo_copy(sp + 1).start())

    def attend(h, r0):
        e = r0 + rb
        q = PJ[r0:e, o_q + h * KEY_DIM:o_q + (h + 1) * KEY_DIM]
        k = PJ[0:e, h * KEY_DIM:(h + 1) * KEY_DIM]
        v = PJ[0:e, o_v + h * VALUE_DIM:o_v + (h + 1) * VALUE_DIM]
        s = mm_t(q, k)
        ti = lax.broadcasted_iota(jnp.int32, (rb, rb), 0)
        si = lax.broadcasted_iota(jnp.int32, (rb, rb), 1)
        rm = RM[h, r0:e, :]
        w = shifted[h:h + 1, 0:e] - jnp.concatenate([rm] * (e // 128), axis=1)
        diag = jnp.where(ti >= si, w[:, r0:e], NEG)
        w = jnp.concatenate([w[:, 0:r0], diag], axis=1) if r0 else diag
        mix = s * jnp.exp(w)
        DEN[h, r0:e, :] = jnp.broadcast_to(jnp.sum(mix, axis=1, keepdims=True), (rb, 128))
        NUM[r0:e, h * VALUE_DIM:(h + 1) * VALUE_DIM] = mm(mix.astype(BF16), v)

    def conv_finish():
        @pl.when(sp > 0)
        def _():
            halo_copy(sp).wait_recv()
            PROD[0:8, :] = halo_in[...].astype(F32)[8:16]

        @pl.when(sp == 0)
        def _():
            PROD[0:8, :] = jnp.zeros((8, channels), F32)

        tap = taps[:, pl.ds(pl.multiple_of(tp * channels, 128), channels)]
        for r0 in range(0, T, rb):
            f = tap[0:1] * PROD[6 + r0:6 + r0 + rb, :]
            f = f + tap[1:2] * PROD[7 + r0:7 + r0 + rb, :]
            f = f + tap[2:3] * PROD[8 + r0:8 + r0 + rb, :]
            gate = PJ[r0:r0 + rb, o_c:o_c + channels].astype(F32)
            CB[r0:r0 + rb, :] = (gate * f).astype(BF16)

    cw = D // RS_CHUNKS
    chips = [y] + [lax.rem(y + k, n_y) for k in range(1, n_y)]
    order = list(range(1, n_y)) + [0]

    def conv_copy(idx):
        return remote(PSC.at[rows_of(2 * chips[idx] + 1 - core), :], DRC.at[idx], s_sem, cd_r.at[idx],
                      to_tp=partner)

    def conv_out(idx, q):
        rr = chip_rows(chips[idx])
        for j in range(q * RS_CHUNKS // 2, (q + 1) * RS_CHUNKS // 2):
            cols = slice(j * cw, (j + 1) * cw)
            PSC[rr, cols] = mm(CB[rr, :], WO[vw:, cols]).astype(BF16)
        if q == 1:
            conv_copy(idx).start()

    early = EARLY * cw

    def early_copy(k):
        return remote(YC.at[k - 1], YCR.at[k - 1], s_sem, yc_r.at[k - 1],
                      to_tp=lax.rem(y + k, n_y) * 2 + core)

    def conv_early():
        for k in range(1, n_y):
            conv_copy(k).wait_recv()
            mine = rows_of(2 * chips[k] + core)
            s = PSC[mine, 0:early].astype(F32) + DRC[k, :, 0:early].astype(F32)
            YC[k - 1] = s.astype(BF16)
            early_copy(k).start()

    work_running_max()
    project_far(2, rest_cols)
    work_product()
    for h in range(heads):
        for r0 in range(0, T, rb):
            attend(h, r0)
    pass_on(0, 10)
    pass_on(1, 10)
    conv_finish()
    for c in out_copies:
        c.wait()
    for idx in order[:-1]:
        for q in range(2):
            conv_out(idx, q)
    pass_on(2, 10)
    for idx in order[-1:]:
        for q in range(2):
            conv_out(idx, q)
    conv_early()
    pass_rest()

    parts = [(0, EARLY), (EARLY, RS_CHUNKS // 2), (RS_CHUNKS // 2, RS_CHUNKS)]
    per_chip = -(-2 * R // 128)

    def mem_copy(idx, q):
        cols = pl.ds(parts[q][0] * cw, (parts[q][1] - parts[q][0]) * cw)
        return remote(PSM.at[rows_of(2 * chips[idx] + 1 - core), cols], DRM.at[idx, :, cols],
                      s_sem, rd_r.at[idx, q], to_tp=partner)

    def mem_out(idx, q):
        rr = chip_rows(chips[idx])
        for j in range(*parts[q]):
            cols = slice(j * cw, (j + 1) * cw)
            PSM[rr, cols] = mm(MO[rr, :], WO[0:vw, cols]).astype(BF16)
        mem_copy(idx, q).start()

    sq_out[...] = jnp.zeros_like(sq_out)
    sq = [None] * n_y
    for h in range(heads):
        end_wait(h)
        wts = weights(h, x_in)
        c_mem = joined(h, *wts[:3], 0, KEY_DIM)
        c_norm, cmax = wts[3], wts[4]
        hi = c_mem.astype(BF16)
        lo = (c_mem - hi.astype(F32)).astype(BF16)
        two = jnp.concatenate([hi, lo], axis=0)
        n_col = jnp.broadcast_to(c_norm, (128, 128)).T
        n_hi = n_col.astype(BF16)
        n_lo = (n_col - n_hi.astype(F32)).astype(BF16)
        n_two = jnp.concatenate([n_hi, n_lo], axis=0)
        for idx in order:
            rr = chip_rows(chips[idx])
            q = PJ[rr, o_q + h * KEY_DIM:o_q + (h + 1) * KEY_DIM]
            qq = jnp.concatenate([q, q], axis=1)
            fm = mm(qq, two)
            fn = mm(qq, n_two)
            m0 = RM[h, rr, :]
            m = jnp.maximum(m0, cmax)
            k0 = jnp.exp(m0 - m)
            k1 = jnp.exp(cmax - m) * q_scale
            den = k0 * DEN[h, rr, :] + k1 * fn
            inv = 1.0 / jnp.maximum(jnp.abs(den), 1.0)
            k0, k1 = k0 * inv, k1 * inv
            cols = slice(h * VALUE_DIM, (h + 1) * VALUE_DIM)
            mo = (jnp.concatenate([k0, k0], axis=1) * NUM[rr, cols]
                  + jnp.concatenate([k1, k1], axis=1) * fm)
            MO[rr, cols] = mo.astype(BF16)
            s2 = mo * mo
            s2 = s2[:, 0:128] + s2[:, 128:256]
            sq[idx] = s2 if sq[idx] is None else sq[idx] + s2
            if h == heads - 1 and idx > 0:
                mem_out(idx, 0)
    for idx in range(n_y):
        for i in range(per_chip):
            n = min(128, 2 * R - i * 128)
            row = jnp.sum(sq[idx][i * 128:i * 128 + n].T, axis=0, keepdims=True)
            sq_out[pl.ds(chips[idx] * per_chip + i, 1), 0:n] = row
    for k in range(1, n_tp):
        cp = remote(sq_out, sq_in.at[k - 1], s_sem, sq_r, to_tp=lax.rem(tp + k, n_tp))
        cp.start()
        sends.append(cp)

    def cols_of(j):
        return pl.ds(j * cw, cw)

    def y_copy(k, j):
        return remote(YS.at[k - 1, :, cols_of(j)], YR.at[k - 1, :, cols_of(j)], s_sem,
                      ry_r.at[k - 1, j], to_tp=lax.rem(y + k, n_y) * 2 + core)

    def mem_sum(idx, j):
        cols = slice(j * cw, (j + 1) * cw)
        mine = rows_of(2 * chips[idx] + core)
        return PSM[mine, cols].astype(F32) + DRM[idx, :, cols].astype(F32)

    for idx in order[:-1]:
        mem_out(idx, 1)
    for k in range(1, n_y):
        mem_copy(k, 0).wait_recv()
        for j in range(EARLY):
            YS[k - 1, :, j * cw:(j + 1) * cw] = mem_sum(k, j).astype(BF16)
            y_copy(k, j).start()
    for idx in order[:-1]:
        mem_out(idx, 2)
    for q in range(2):
        mem_out(0, q)

    tot = sq_out[...]
    remote(sq_in, sq_in, s_sem, sq_r, to_tp=partner).wait_recv()
    for k in range(1, n_tp):
        tot = tot + sq_in[k - 1]
    r_scale = lax.rsqrt(tot / float(width) + EPS)
    for c in range(n_y):
        for i in range(per_chip):
            n = min(128, 2 * R - i * 128)
            at = c * 2 * R + i * 128
            RC[at:at + n, :] = jnp.broadcast_to(r_scale[c * per_chip + i:c * per_chip + i + 1, 0:n], (128, n)).T

    def row_scale(idx):
        return jnp.concatenate([RC[rows_of(2 * chips[idx] + core), :]] * (cw // 128), axis=1)

    def chip_sum(idx, j):
        cols = slice(j * cw, (j + 1) * cw)
        mine = rows_of(2 * chips[idx] + core)
        s = PSC[mine, cols].astype(F32) + DRC[idx, :, cols].astype(F32)
        return s + mem_sum(idx, j) * row_scale(idx)

    for k in range(1, n_y):
        for q in range(1, 3):
            mem_copy(k, q).wait_recv()
        for j in range(EARLY, RS_CHUNKS):
            YS[k - 1, :, j * cw:(j + 1) * cw] = chip_sum(k, j).astype(BF16)
            y_copy(k, j).start()
    mem_out(0, 2)
    conv_copy(0).wait_recv()
    for q in range(3):
        mem_copy(0, q).wait_recv()
    for k in range(1, n_y):
        early_copy(k).wait_recv()
    for j in range(RS_CHUNKS):
        s = chip_sum(0, j)
        for k in range(1, n_y):
            y_copy(k, j).wait_recv()
            got = YR[k - 1, :, j * cw:(j + 1) * cw].astype(F32)
            if j < EARLY:
                got = got * row_scale(0) + YCR[k - 1, :, j * cw:(j + 1) * cw].astype(F32)
            s = s + got
        out[:, j * cw:(j + 1) * cw] = s.astype(BF16)

    for cp in sends:
        cp.wait_send()
    own.wait_send()
    for h in range(heads):
        for p in range(PARTS + 1):
            group_sends(lambda k, h=h, p=p: group_copies(k, h, p).wait_send())

            @pl.when(zg < A - 1)
            def _(h=h, p=p):
                chain_copy(h, p).wait_send()
    pl.when(sp < n_sp - 1)(lambda: halo_copy(sp + 1).wait_send())
    for idx in range(n_y):
        conv_copy(idx).wait_send()
        for q in range(3):
            mem_copy(idx, q).wait_send()
    for k in range(1, n_y):
        early_copy(k).wait_send()
        for j in range(RS_CHUNKS):
            y_copy(k, j).wait_send()


def per_device(
    n_sp, n_tp,
    tokens, in_gain, w_query, w_key, w_value, w_input_gate, w_forget_gate, forget_bias,
    forget_extra, w_conv_gate, w_conv_left, w_conv_right, conv_taps, first_memory, first_norm,
    w_out_memory, w_out_conv,
):
    heads = w_query.shape[1] // KEY_DIM
    channels = w_conv_gate.shape[1]
    R, D = tokens.shape
    T = R * n_tp
    n_y = n_tp // 2
    qk, vw = heads * KEY_DIM, heads * VALUE_DIM
    total = 2 * qk + vw + 128 + 3 * channels
    n_heads = w_input_gate.shape[1]
    B = group_size(n_sp)
    hbm = pl.BlockSpec(memory_space=pl.ANY)
    V, dma = pltpu.VMEM, pltpu.SemaphoreType.DMA
    ny1 = n_y - 1
    np_ = len(gather_pieces(R))
    sq_rows = -(-(n_y * -(-2 * R // 128)) // 8) * 8
    early = EARLY * D // RS_CHUNKS
    return pl.pallas_call(
        functools.partial(kernel, n_sp, n_tp, heads, channels, n_heads * VALUE_DIM),
        out_shape=pltpu.VMEM((R, D), BF16),
        in_specs=[hbm] * 17,
        out_specs=pl.BlockSpec(memory_space=pltpu.VMEM),
        scratch_shapes=[
            V((R, D), BF16), V((1, D), F32), V((n_heads, D), BF16), V((n_heads, D), BF16),
            pltpu.SMEM((n_heads,), F32), V((heads, T), F32), V((TAPS, n_tp * channels), F32),
            V((heads, KEY_DIM, VALUE_DIM), F32), V((heads, KEY_DIM), F32),
            V((D, total), BF16), V((vw + channels, D), BF16), V((T, D), BF16), V((T, total), BF16),
            V((T, 128), F32), V((heads, T, 128), F32), V((T, vw), F32), V((heads, T, 128), F32),
            V((T, vw), BF16), V((T, channels), BF16), V((8 + T, channels), F32),
            V((16, channels), BF16), V((16, channels), BF16),
            V((B, heads, KEY_DIM, VALUE_DIM), BF16), V((B, heads, 8, 128), F32),
            V((heads, KEY_DIM, VALUE_DIM), BF16), V((heads, KEY_DIM, VALUE_DIM), BF16),
            V((heads, 8, 128), F32), V((heads, 8, 128), F32), V((heads, 8 * -(-(B + 1) // 8), 128), F32),
            V((sq_rows, 128), F32), V((n_tp - 1, sq_rows, 128), F32), V((T, 128), F32),
            V((T, D), BF16), V((T, D), BF16), V((n_y, R, D), BF16), V((n_y, R, D), BF16),
            V((ny1, R, D), BF16), V((ny1, R, D), BF16),
            V((ny1, R, early), BF16), V((ny1, R, early), BF16),
            dma((7,)), dma, dma, dma((ny1, np_)), dma((ny1, np_)), dma((B - 1, heads, PARTS + 1)),
            dma((heads, PARTS + 1)), dma, dma, dma((n_y,)), dma((n_y, 3)), dma((ny1, RS_CHUNKS)), dma((ny1,)),
            pltpu.SemaphoreType.REGULAR,
        ],
        compiler_params=pltpu.CompilerParams(
            collective_id=0, has_side_effects=True, vmem_limit_bytes=60 * 1024 * 1024),
        name="layer",
    )(
        tokens, in_gain.reshape(1, D), w_key, w_value, w_query, w_conv_gate, w_conv_left,
        w_conv_right, w_input_gate.T, w_forget_gate.T, forget_bias, forget_extra.T, conv_taps, first_memory, first_norm,
        w_out_memory, w_out_conv,
    )


def solution(mesh):
    in_specs = (
        P(("sp", "tp"), None), P(), P(None, "tp"), P(None, "tp"), P(None, "tp"), P(), P(), P(),
        P("sp", "tp"), P(None, "tp"), P(None, "tp"), P(None, "tp"), P(), P("tp", None, None),
        P("tp", None), P("tp", None), P("tp", None),
    )
    return jax.shard_map(
        functools.partial(per_device, mesh.shape["sp"], mesh.shape["tp"]),
        mesh=mesh, in_specs=in_specs, out_specs=P(("sp", "tp"), None), check_vma=False,
    )
```
